32 devices in a mesh: ep: 16 (over z, y, x), tp: 2 (over core).
Axes of the slice: x: 2, y: 2, z: 4, core: 2. Of those that a mesh axis runs over, the one named last changes fastest.
Arguments:
- tokens: bfloat16 [8192, 2048], P(('ep', 'tp')), may hold values from -6 to 6
- norm_gain: float32 [2048], replicated, may hold values from 0.1 to 1.9
- expert_ids: int32 [8192, 2], P(('ep', 'tp')), may hold values from 0 to 15, all different within a row; in each aligned block of 256 rows (0 to 255, 256 to 511, ...) at most 48 rows name the same one
- route_weights: float32 [8192, 2], P(('ep', 'tp')), may hold values from 0.2 to 1.2
- expert_gate: bfloat16 [16, 2048, 512], P('ep', None, 'tp'), may hold values from -0.125 to 0.125
- expert_up: bfloat16 [16, 2048, 512], P('ep', None, 'tp'), may hold values from -0.125 to 0.125
- expert_down: bfloat16 [16, 512, 2048], P('ep', 'tp'), may hold values from -0.25 to 0.25
- shared_gate: bfloat16 [2048, 512], P(None, 'tp'), may hold values from -0.125 to 0.125
- shared_up: bfloat16 [2048, 512], P(None, 'tp'), may hold values from -0.125 to 0.125
- shared_down: bfloat16 [512, 2048], P('tp'), may hold values from -0.25 to 0.25
Outputs:
- mixed: bfloat16 [8192, 2048], P(('ep', 'tp'))
The draws below stay inside these ranges and needn't reach their ends.
Inputs may be any that keep to these rules, and one draw needn't show every extreme that they name: `expert_ids`: each token names 2 different experts. Among the tokens of one device (aligned blocks of 256 rows) no expert is named by more than 48 tokens, and in every block some expert is named by exactly 48.
All inputs are finite; a program needn't handle non-finite values.
Results may differ from the reference program's by a relative error of at most 0.0075.
Values may be sent and summed in bfloat16 or wider, within the bound.
A program may use at most 64 MiB of HBM per device.

```python
import math
import jax
import jax.numpy as jnp
import numpy as np
from jax import lax

D = 2048
DE = 512
DS = 512
TOP_K = 2
TOK_DEV = 256
EXPERTS = 16
CAP = 48
TOKENS = 8192
N_EP = 16
N_TP = 2


def block_scale(key, shape, pieces, smallest, top_value):
    factor_of, own = 1.0, jax.random.fold_in(key, 6)
    for axis_at, blocks in pieces:
        draws = jnp.exp(jax.random.uniform(jax.random.fold_in(own, axis_at), (blocks,), jnp.float32, smallest / len(pieces), top_value / len(pieces)))
        factor_of = factor_of * jnp.repeat(draws, shape[axis_at] // blocks).reshape([-1 if axis == axis_at else 1 for axis in range(len(shape))])
    return factor_of


def assign_block(key, own, number, rows, amount, top, most, skew):
    order = jax.random.permutation(key, amount)
    heavy_load, ordinary = load_shares(amount, rows * top, most, skew, True), load_shares(amount, rows * top, most, skew, False)
    places = jnp.arange(amount)

    def named(lengths, offset_by):
        used = int((lengths > 0).sum())
        fixed = max(1, used // 4)
        moved = fixed + (places - fixed + offset_by * (used - fixed)) % max(1, amount - fixed)
        return jnp.zeros((amount,), jnp.int32).at[order[jnp.where(places < fixed, places, moved)]].set(jnp.asarray(lengths, jnp.int32))

    lengths = jnp.where(number % 4 == 0, named(heavy_load, number // 4), named(ordinary, number - number // 4 - 1))
    mixed = jax.random.permutation(jax.random.fold_in(own, 3), amount)
    giver, sink = mixed[0:amount // 2 * 2:2], mixed[1:amount // 2 * 2:2]
    slack = jnp.minimum(lengths[giver] - 1, most - lengths[sink]) // 2
    slack = jnp.where((giver == order[0]) | (sink == order[0]) | (lengths[sink] == 0), 0, jnp.maximum(slack, 0))
    moved = jax.random.randint(jax.random.fold_in(own, 4), (amount // 2,), 0, 1 << 20) % (slack + 1)
    lengths = lengths.at[giver].add(-moved).at[sink].add(moved)
    items = jnp.searchsorted(jnp.cumsum(lengths), jnp.arange(rows * top), side="right").astype(jnp.int32)
    grid = items.reshape(top, rows).T
    grid = grid[jax.random.permutation(jax.random.fold_in(own, 1), rows)]
    offset_by = jax.random.randint(jax.random.fold_in(own, 2), (rows, 1), 0, top)
    return jnp.take_along_axis(grid, (jnp.arange(top)[None, :] + offset_by) % top, axis=1)


def load_shares(number_of, total, limit, skew, full):
    portions = [(1 << 20) // math.isqrt(standing ** skew) + 1 for standing in range(1, number_of + 1)]
    largest = limit if full else min(limit, max(-(-total // number_of), total * portions[0] // sum(portions)))
    least = 1 if total - largest >= number_of - 1 else 0
    holding, spare = [largest] + [least] * (number_of - 1), total - largest - least * (number_of - 1)
    while spare > 0:
        movable = [i for i in range(1, number_of) if holding[i] < largest] or [i for i in range(1, number_of) if holding[i] < limit]
        mass, left = sum([portions[i] for i in movable]), spare
        for i in movable:
            addition = min(limit - holding[i], max(1, left * portions[i] // mass), spare)
            holding[i] = holding[i] + addition
            spare = spare - addition
    return np.array(holding)


def noise(own_key, extent, spread, reach, split=(), kind=jnp.bfloat16):
    gain = block_scale(own_key, extent, split, -0.22, 0.18) if split else 1.0
    array = jax.random.normal(own_key, extent, jnp.float32) * spread * gain
    return jnp.minimum(jnp.maximum(array, -reach), reach).astype(kind)


def setup_inputs(seed: int = 0) -> dict:
    key_of = jax.random.split(jax.random.key(seed), 11)
    tokens = noise(key_of[0], (TOKENS, D), 1.0, 6.0, ((0, 32),))
    norm_gain = jnp.clip(1.0 + 0.18 * jax.random.normal(key_of[1], (D,), jnp.float32), 0.1, 1.9)
    expert_ids_keys = jax.random.split(jax.random.fold_in(key_of[2], 1), TOKENS // TOK_DEV)
    expert_ids_turns = jax.random.permutation(jax.random.fold_in(key_of[2], 3), TOKENS // TOK_DEV)
    expert_ids = jax.vmap(lambda own, number: assign_block(jax.random.fold_in(key_of[2], 2), own, number, TOK_DEV, EXPERTS, TOP_K, CAP, 2))(expert_ids_keys, expert_ids_turns).reshape((TOKENS, TOP_K))
    route_weights = jnp.clip(0.2 + 1 * jax.random.uniform(key_of[3], (TOKENS, TOP_K), jnp.float32) ** block_scale(key_of[3], (TOKENS, TOP_K), ((0, 32),), -0.2, 0.2), 0.2, 1.2)
    expert_gate = noise(key_of[4], (EXPERTS, D, DE), D ** -0.5, 0.125, ((0, 16), (2, 2)))
    expert_up = noise(key_of[5], (EXPERTS, D, DE), D ** -0.5, 0.125, ((0, 16), (2, 2)))
    expert_down = noise(key_of[6], (EXPERTS, DE, D), DE ** -0.5, 0.25, ((0, 16), (1, 2)))
    shared_gate = noise(key_of[7], (D, DS), D ** -0.5, 0.125, ((1, 2),))
    shared_up = noise(key_of[8], (D, DS), D ** -0.5, 0.125, ((1, 2),))
    shared_down = noise(key_of[9], (DS, D), DS ** -0.5, 0.25, ((0, 2),))
    return {"tokens": tokens, "norm_gain": norm_gain, "expert_ids": expert_ids, "route_weights": route_weights, "expert_gate": expert_gate, "expert_up": expert_up, "expert_down": expert_down, "shared_gate": shared_gate, "shared_up": shared_up, "shared_down": shared_down}


epsilon = 1e-06

def normalize(tokens, norm_gain):
    values = tokens.astype(jnp.float32)
    factor = lax.rsqrt(lax.optimization_barrier(jnp.mean(values * values, axis=1, keepdims=True)) + epsilon)
    return (values * factor * norm_gain[None, :]).astype(jnp.bfloat16)

def halves(row_block, gate_w, up_w, down_w):
    half_width = gate_w.shape[1] // N_TP
    summed = jnp.zeros((row_block.shape[0], down_w.shape[1]), jnp.float32)
    for portion in range(N_TP):
        first = portion * half_width
        gate_value = jnp.dot(row_block, gate_w[:, first:first + half_width], preferred_element_type=jnp.float32)
        up_value = jnp.dot(row_block, up_w[:, first:first + half_width], preferred_element_type=jnp.float32)
        hidden = (jax.nn.silu(gate_value) * up_value).astype(jnp.bfloat16)
        partial_value = jnp.dot(hidden, down_w[first:first + half_width], preferred_element_type=jnp.float32)
        rounded = lax.optimization_barrier(partial_value.astype(jnp.bfloat16))
        summed = summed + rounded.astype(jnp.float32)
    return summed

def reference(tokens, norm_gain, expert_ids, route_weights, expert_gate, expert_up, expert_down, shared_gate, shared_up, shared_down):
    normed = normalize(tokens, norm_gain)
    total_rows = tokens.shape[0]
    shared_out = halves(normed, shared_gate, shared_up, shared_down)
    flat_ids = expert_ids.reshape(-1).astype(jnp.int32)
    assigned = flat_ids.shape[0]
    ordering = jnp.argsort(flat_ids, stable=True).astype(jnp.int32)
    counts = jnp.bincount(flat_ids, length=EXPERTS).astype(jnp.int32)
    starts = (jnp.cumsum(counts) - counts).astype(jnp.int32)
    most_rows = N_EP * N_TP * CAP
    padded = jnp.concatenate([normed, jnp.zeros((1, D), jnp.bfloat16)], axis=0)
    flat_weights = route_weights.reshape(-1)

    def per_expert(totals, expert):
        slot_range = jnp.arange(most_rows, dtype=jnp.int32)
        filled = slot_range < counts[expert]
        row_index = jnp.minimum(starts[expert] + slot_range, assigned - 1)
        assign = jnp.where(filled, ordering[row_index], assigned)
        token_index = (assign // TOP_K).astype(jnp.int32)
        row_block = padded[token_index]
        expert_out = halves(row_block, expert_gate[expert], expert_up[expert], expert_down[expert]).astype(jnp.bfloat16)
        weight_rows = jnp.where(filled, flat_weights[jnp.minimum(assign, assigned - 1)], jnp.float32(0.0))
        totals = totals.at[token_index].add(expert_out.astype(jnp.float32) * weight_rows[:, None])
        return (totals, None)
    totals, _ = lax.scan(per_expert, jnp.zeros((total_rows + 1, D), jnp.float32), jnp.arange(EXPERTS, dtype=jnp.int32))
    routed = totals[:total_rows]
    return (routed + shared_out).astype(jnp.bfloat16)
```

```python
import functools

import jax
import jax.numpy as jnp
from jax import lax
from jax.experimental import pallas as pl
from jax.experimental.pallas import tpu as pltpu
from jax.sharding import PartitionSpec as P

epsilon = 1e-06
MESH = pl.DeviceIdType.MESH


def toggled(index, step, size):
    total, bit = 0, 1
    while bit < size:
        total = total + bit * ((index // bit + step // bit) % 2)
        bit *= 2
    return total


def gated_sum(rows, gate_w, up_w, down_w):
    total = None
    for half in range(gate_w.shape[0]):
        gate_value = jnp.dot(rows, gate_w[half], preferred_element_type=jnp.float32)
        up_value = jnp.dot(rows, up_w[half], preferred_element_type=jnp.float32)
        hidden = (gate_value / (1.0 + jnp.exp(-gate_value)) * up_value).astype(jnp.bfloat16)
        term = jnp.dot(hidden, down_w[half], preferred_element_type=jnp.float32)
        total = term if total is None else total + term
    return total


def slot_rows(meta, me, steps):
    count = meta.shape[1]
    relative = meta[0:2, :].astype(jnp.int32) ^ me
    step_of = lax.broadcasted_iota(jnp.int32, (steps, count), 0)
    named = (step_of == relative[0:1, :]) | (step_of == relative[1:2, :])
    row_at = lax.broadcasted_iota(jnp.int32, (count, count), 0)
    col_at = lax.broadcasted_iota(jnp.int32, (count, count), 1)
    before = jnp.where(row_at < col_at, 1.0, 0.0).astype(jnp.bfloat16)
    slots = jnp.dot(
        jnp.where(named, 1.0, 0.0).astype(jnp.bfloat16), before, preferred_element_type=jnp.float32
    ).astype(jnp.int32)
    return jnp.where(named, slots, -1)


def picks(slots, steps, capacity):
    slot_at = lax.broadcasted_iota(jnp.int32, (capacity, slots.shape[1]), 0)
    return jnp.concatenate(
        [
            jnp.where(slot_at == slots[step : step + 1, :], 1.0, 0.0).astype(jnp.bfloat16)
            for step in steps
        ],
        axis=0,
    )


def slot_places(meta, me, capacity):
    count = meta.shape[1]
    turned = jnp.transpose(meta)
    relative = turned[:, 0:2].astype(jnp.int32) ^ me
    expert_at = lax.broadcasted_iota(jnp.int32, (count, 128), 1)
    row_at = lax.broadcasted_iota(jnp.int32, (count, count), 0)
    col_at = lax.broadcasted_iota(jnp.int32, (count, count), 1)
    chosen = [expert_at == relative[:, j : j + 1] for j in range(2)]
    after = jnp.where(row_at > col_at, 1.0, 0.0).astype(jnp.bfloat16)
    counted = jnp.dot(
        after,
        jnp.where(chosen[0] | chosen[1], 1.0, 0.0).astype(jnp.bfloat16),
        preferred_element_type=jnp.float32,
    )
    places = [
        relative[:, j : j + 1] * capacity
        + jnp.sum(jnp.where(chosen[j], counted, 0.0), axis=1, keepdims=True).astype(jnp.int32)
        for j in range(2)
    ]
    return places, [turned[:, 2 + j : 3 + j] for j in range(2)]


def weight_matrix(places, weights, first, amount):
    at = lax.broadcasted_iota(jnp.int32, (places[0].shape[0], amount), 1) + first
    scale = jnp.where(at == places[0], weights[0], 0.0) + jnp.where(
        at == places[1], weights[1], 0.0
    )
    upper = scale.astype(jnp.bfloat16)
    return upper, (scale - upper.astype(jnp.float32)).astype(jnp.bfloat16)


def weighted(pair, block):
    return jnp.dot(pair[0], block, preferred_element_type=jnp.float32) + jnp.dot(
        pair[1], block, preferred_element_type=jnp.float32
    )


ORDER = "1S2A3B4F5XGabYN"


def layer_kernel(
    peers,
    capacity,
    pieces,
    tokens,
    gain,
    meta,
    expert_gate,
    expert_up,
    expert_down,
    shared_gate,
    shared_up,
    shared_down,
    mixed,
    gate_all,
    up_all,
    down_all,
    s_gate_all,
    s_up_all,
    s_down_all,
    normed,
    outgoing,
    near_in,
    far_in,
    near_out,
    far_out,
    returned,
    total,
    relay_in,
    meta_in,
    picked,
    relay_out,
    relay_back,
    sums_out,
    sums_in,
    weight_local,
    weight_send,
    weight_recv,
    out_send,
    out_recv,
    back_send,
    back_recv,
    block_send,
    block_recv,
    meta_send,
    meta_recv,
    relay_send,
    relay_recv,
    home_send,
    home_recv,
    sums_send,
    sums_recv,
):
    me = lax.axis_index("ep")
    core = lax.axis_index("tp")
    sibling = 1 - core
    width = tokens.shape[1]
    piece = width // pieces
    half, quarter = peers // 2, peers // 4
    inner = ((me // quarter + 1) // 2) % 2
    turns = (half, half + quarter)

    def at_step(step):
        return (toggled(me, step, peers), core)

    def columns(c):
        return pl.ds(c * piece, piece)

    def remote(source, target, send, recv, place):
        return pltpu.make_async_remote_copy(
            src_ref=source,
            dst_ref=target,
            send_sem=send,
            recv_sem=recv,
            device_id=place,
            device_id_type=MESH,
        )

    barrier = pltpu.get_barrier_semaphore()
    greeted = range(1, peers)
    pl.semaphore_signal(barrier, inc=1, device_id=(me, sibling), device_id_type=MESH)
    for step in greeted:
        pl.semaphore_signal(barrier, inc=1, device_id=at_step(step), device_id_type=MESH)
    sources = (
        (shared_gate, s_gate_all),
        (shared_up, s_up_all),
        (shared_down, s_down_all),
        (expert_gate, gate_all),
        (expert_up, up_all),
        (expert_down, down_all),
    )
    local = [
        pltpu.make_async_copy(source, target.at[core], weight_local.at[i])
        for i, (source, target) in enumerate(sources)
    ]
    swaps = [
        remote(source, target.at[core], weight_send.at[i], weight_recv.at[i], (me, sibling))
        for i, (source, target) in enumerate(sources)
    ]
    for copy in local:
        copy.start()

    values = tokens[...].astype(jnp.float32)
    factor = lax.rsqrt(jnp.mean(values * values, axis=1, keepdims=True) + epsilon)
    normed[...] = (values * factor * gain[...]).astype(jnp.bfloat16)

    gateway = at_step(half + quarter * inner)
    meta_copy = remote(meta, meta_in.at[inner], meta_send.at[0], meta_recv.at[inner], gateway)

    def block_copy(c):
        return remote(
            normed.at[:, columns(c)],
            relay_in.at[inner, :, columns(c)],
            block_send.at[c],
            block_recv.at[inner, c],
            gateway,
        )

    def send_block():
        for c in range(pieces):
            block_copy(c).start()

    def dispatch(step):
        return remote(
            outgoing.at[step], near_in.at[step], out_send.at[step], out_recv.at[step], at_step(step)
        )

    def give_back(step):
        return remote(
            near_out.at[step],
            returned.at[step],
            back_send.at[step],
            back_recv.at[step],
            at_step(step),
        )

    def relay(side, k, c):
        return remote(
            relay_out.at[side, k, :, columns(c)],
            far_in.at[side, k % quarter, :, columns(c)],
            relay_send.at[side * half + k, c],
            relay_recv.at[side * quarter + k % quarter, c],
            at_step(k),
        )

    def home(side, j):
        k = j + quarter * (1 - inner)
        return remote(
            far_out.at[side, j],
            relay_back.at[side, k],
            home_send.at[side * quarter + j],
            home_recv.at[side * half + k],
            at_step(k),
        )

    def sums(side, c):
        return remote(
            sums_out.at[side, :, columns(c)],
            sums_in.at[:, columns(c)],
            sums_send.at[side * pieces + c],
            sums_recv.at[c],
            at_step(turns[side]),
        )

    def on_inner(action):
        pl.when(inner == 1)(action)

    pl.semaphore_wait(barrier, len(greeted) + 1)
    meta_copy.start()
    on_inner(send_block)

    slots = slot_rows(meta[...], me, half)

    def send_slots(first):
        rows = jnp.dot(
            picks(slots, range(first, first + quarter), capacity),
            normed[...],
            preferred_element_type=jnp.float32,
        ).astype(jnp.bfloat16)
        for i in range(quarter):
            block = rows[i * capacity : (i + 1) * capacity]
            if first + i == 0:
                near_in[0] = block
            else:
                outgoing[first + i] = block
                dispatch(first + i).start()

    send_slots(quarter)
    send_slots(0)
    pl.when(inner == 0)(send_block)
    for copy in swaps:
        copy.start()

    def open_side(side):
        remote(
            meta, meta_in.at[side], meta_send.at[0], meta_recv.at[side], at_step(turns[side])
        ).wait_recv()
        picked[side] = picks(slot_rows(meta_in[side], me, half), range(half), capacity)

    def pass_on(side, c):
        remote(
            normed.at[:, columns(c)],
            relay_in.at[side, :, columns(c)],
            block_send.at[c],
            block_recv.at[side, c],
            at_step(turns[side]),
        ).wait_recv()
        rows = jnp.dot(
            picked[side], relay_in[side, :, columns(c)], preferred_element_type=jnp.float32
        ).astype(jnp.bfloat16)
        far_in[side, 0, :, columns(c)] = rows[:capacity]
        for k in range(half - 1, 0, -1):
            relay_out[side, k, :, columns(c)] = rows[k * capacity : (k + 1) * capacity]
            relay(side, k, c).start()

    def pass_some(side, chunks):
        def action():
            if chunks[0] == 0:
                open_side(side)
            for c in chunks:
                pass_on(side, c)

        on_inner(action)

    def near(group):
        steps = range(group * quarter, (group + 1) * quarter)
        for step in steps:
            if step > 0:
                dispatch(step).wait_recv()
        block = near_in[group * quarter : (group + 1) * quarter].reshape(quarter * capacity, width)
        out = gated_sum(block, gate_all, up_all, down_all).astype(jnp.bfloat16)
        for i, step in enumerate(steps):
            part = out[i * capacity : (i + 1) * capacity]
            if step == 0:
                returned[0] = part
            else:
                near_out[step] = part

    def near_send(group):
        for step in range(group * quarter, (group + 1) * quarter):
            if step > 0:
                give_back(step).start()

    def far_wait(side, j):
        for c in range(pieces):
            remote(
                relay_out.at[side, 1, :, columns(c)],
                far_in.at[side, j, :, columns(c)],
                relay_send.at[side * half + 1, c],
                relay_recv.at[side * quarter + j, c],
                at_step(1),
            ).wait_recv()

    def far(side):
        pl.when(inner == 0)(lambda: far_wait(side, 0))
        for j in range(1, quarter):
            far_wait(side, j)
        block = far_in[side].reshape(quarter * capacity, width)
        out = gated_sum(block, gate_all, up_all, down_all).astype(jnp.bfloat16)
        for j in range(quarter - 1, -1, -1):
            part = out[j * capacity : (j + 1) * capacity]
            far_out[side, j] = part
            if j == 0:

                @pl.when(inner == 0)
                def _():
                    home(side, 0).start()

                @pl.when(inner == 1)
                def _():
                    relay_back[side, 0] = far_out[side, 0]
            else:
                home(side, j).start()

    def send_sums(side):
        places, scales = slot_places(meta_in[side], me, capacity)
        pair = weight_matrix(places, scales, 0, half * capacity)
        for k in range(1, half):
            remote(
                far_out.at[side, 1],
                relay_back.at[side, k],
                home_send.at[side * quarter + 1],
                home_recv.at[side * half + k],
                at_step(k),
            ).wait_recv()
        for c in range(pieces):
            block = relay_back[side, :, :, columns(c)]
            sums_out[side, :, columns(c)] = weighted(
                pair, block.reshape(half * capacity, piece)
            ).astype(jnp.bfloat16)
            sums(side, c).start()

    def shared():
        for i in range(len(sources)):
            local[i].wait()
            swaps[i].wait()
        total[...] = gated_sum(normed[...], s_gate_all, s_up_all, s_down_all)

    def near_total():
        places, scales = slot_places(meta[...], me, capacity)
        pair = weight_matrix(places, scales, 0, half * capacity)
        for step in range(1, half):
            give_back(step).wait_recv()
        total[...] += weighted(pair, returned[...].reshape(half * capacity, width))

    actions = {
        "S": shared,
        "A": lambda: near(0),
        "B": lambda: near(1),
        "a": lambda: near_send(0),
        "b": lambda: near_send(1),
        "F": lambda: far(1),
        "G": lambda: far(0),
        "1": lambda: pass_some(1, (0, 1)),
        "2": lambda: pass_some(1, (2,)),
        "3": lambda: pass_some(1, (3,)),
        "4": lambda: pass_some(0, (0, 1)),
        "5": lambda: pass_some(0, (2, 3)),
        "X": lambda: on_inner(lambda: send_sums(1)),
        "Y": lambda: on_inner(lambda: send_sums(0)),
        "N": near_total,
    }
    for name in ORDER:
        actions[name]()

    for c in range(pieces):
        remote(
            sums_out.at[0, :, columns(c)],
            sums_in.at[:, columns(c)],
            sums_send.at[c],
            sums_recv.at[c],
            gateway,
        ).wait_recv()
        mixed[:, columns(c)] = (
            total[:, columns(c)] + sums_in[:, columns(c)].astype(jnp.float32)
        ).astype(jnp.bfloat16)

    meta_copy.wait_send()
    for c in range(pieces):
        block_copy(c).wait_send()
    for step in range(1, half):
        dispatch(step).wait_send()
        give_back(step).wait_send()
    for side in range(2):
        pl.when(inner == 0)(lambda: home(side, 0).wait_send())
        for j in range(1, quarter):
            home(side, j).wait_send()

    @pl.when(inner == 1)
    def _():
        for side in range(2):
            for c in range(pieces):
                sums(side, c).wait_send()
                for k in range(1, half):
                    relay(side, k, c).wait_send()


def kernel_body(
    tokens,
    norm_gain,
    expert_ids,
    route_weights,
    expert_gate,
    expert_up,
    expert_down,
    shared_gate,
    shared_up,
    shared_down,
):
    peers = lax.axis_size("ep")
    halves = lax.axis_size("tp")
    tok_rows, width = tokens.shape
    capacity = 3 * tok_rows * expert_ids.shape[1] // (2 * peers)
    half, quarter, pieces = peers // 2, peers // 4, 4
    vmem = pl.BlockSpec(memory_space=pltpu.VMEM)
    anywhere = pl.BlockSpec(memory_space=pl.ANY)
    weights = (
        expert_gate[0],
        expert_up[0],
        expert_down[0],
        shared_gate,
        shared_up,
        shared_down,
    )
    meta = jnp.concatenate(
        [expert_ids.astype(jnp.float32), route_weights, jnp.zeros((tok_rows, 4), jnp.float32)],
        axis=1,
    ).T

    def rows(*shape):
        return pltpu.VMEM(shape, jnp.bfloat16)

    dma = pltpu.SemaphoreType.DMA
    return pl.pallas_call(
        functools.partial(layer_kernel, peers, capacity, pieces),
        out_shape=jax.ShapeDtypeStruct((tok_rows, width), jnp.bfloat16),
        in_specs=[vmem] * 3 + [anywhere] * 6,
        out_specs=vmem,
        scratch_shapes=[pltpu.VMEM((halves,) + w.shape, w.dtype) for w in weights]
        + [
            rows(tok_rows, width),
            rows(half, capacity, width),
            rows(half, capacity, width),
            rows(2, quarter, capacity, width),
            rows(half, capacity, width),
            rows(2, quarter, capacity, width),
            rows(half, capacity, width),
            pltpu.VMEM((tok_rows, width), jnp.float32),
            rows(2, tok_rows, width),
            pltpu.VMEM((2,) + meta.shape, jnp.float32),
            rows(2, half * capacity, tok_rows),
            rows(2, half, capacity, width),
            rows(2, half, capacity, width),
            rows(2, tok_rows, width),
            rows(tok_rows, width),
        ]
        + [dma((len(weights),))] * 3
        + [dma((half,))] * 4
        + [dma((pieces,)), dma((2, pieces)), dma((1,)), dma((2,))]
        + [dma((2 * half, pieces)), dma((2 * quarter, pieces))]
        + [dma((2 * quarter,)), dma((2 * half,))]
        + [dma((2 * pieces,)), dma((pieces,))],
        compiler_params=pltpu.CompilerParams(
            collective_id=0, has_side_effects=True, vmem_limit_bytes=60 * 1024 * 1024
        ),
        name="layer",
    )(tokens, norm_gain.reshape(1, width), meta, *weights)


def normalize(tokens, norm_gain):
    values = tokens.astype(jnp.float32)
    factor = lax.rsqrt(jnp.mean(values * values, axis=1, keepdims=True) + epsilon)
    return (values * factor * norm_gain[None, :]).astype(jnp.bfloat16)


def round_term(partial_value):
    return lax.optimization_barrier(partial_value.astype(jnp.bfloat16)).astype(jnp.float32)


def gated_rows(row_block, gate_w, up_w):
    gate_value = jnp.dot(row_block, gate_w, preferred_element_type=jnp.float32)
    up_value = jnp.dot(row_block, up_w, preferred_element_type=jnp.float32)
    return (jax.nn.silu(gate_value) * up_value).astype(jnp.bfloat16)


def sliced_term(hidden, down_w):
    return round_term(jnp.dot(hidden, down_w, preferred_element_type=jnp.float32))


def shared_branch(normed, shared_gate, shared_up, shared_down):
    hidden = gated_rows(lax.all_gather(normed, "tp", axis=0, tiled=True), shared_gate, shared_up)
    return lax.psum_scatter(
        sliced_term(hidden, shared_down).astype(jnp.bfloat16), "tp", scatter_dimension=0, tiled=True
    ).astype(jnp.float32)


def body(
    tokens,
    norm_gain,
    expert_ids,
    route_weights,
    expert_gate,
    expert_up,
    expert_down,
    shared_gate,
    shared_up,
    shared_down,
):
    normed = normalize(tokens, norm_gain)
    tok_rows = tokens.shape[0]
    model_width = tokens.shape[1]
    top_count = expert_ids.shape[1]
    ep_size = lax.axis_size("ep")
    experts = expert_gate.shape[0] * ep_size
    capacity = 3 * tok_rows * top_count // (2 * experts)
    assigned = tok_rows * top_count
    gate_one = expert_gate[0]
    up_one = expert_up[0]
    down_one = expert_down[0]
    flat_ids = expert_ids.reshape(-1)
    onehot = (flat_ids[:, None] == jnp.arange(experts, dtype=jnp.int32)[None, :]).astype(
        jnp.bfloat16
    )
    earlier = (jnp.arange(assigned)[:, None] > jnp.arange(assigned)[None, :]).astype(jnp.bfloat16)
    before_count = jnp.dot(earlier, onehot, preferred_element_type=jnp.float32)
    slot_index = jnp.sum(before_count * onehot.astype(jnp.float32), axis=1).astype(jnp.int32)
    position = flat_ids * capacity + slot_index
    owners = (
        jnp.full((experts * capacity,), tok_rows, jnp.int32)
        .at[position]
        .set(jnp.arange(assigned, dtype=jnp.int32) // top_count)
    )
    padded = jnp.concatenate([normed, jnp.zeros((1, model_width), jnp.bfloat16)], axis=0)
    outgoing = padded[owners].reshape(ep_size, capacity, model_width)
    half_slots = capacity // 2
    split_rows = outgoing.reshape(ep_size, 2, half_slots, model_width)
    results = []
    for portion in range(2):
        received = lax.all_to_all(
            split_rows[:, portion], "ep", split_axis=0, concat_axis=0, tiled=True
        )
        hidden = gated_rows(
            lax.all_gather(
                received.reshape(ep_size * half_slots, model_width), "tp", axis=0, tiled=True
            ),
            gate_one,
            up_one,
        )
        summed = lax.psum_scatter(
            sliced_term(hidden, down_one).astype(jnp.bfloat16),
            "tp",
            scatter_dimension=0,
            tiled=True,
        )
        results.append(
            lax.all_to_all(
                summed.reshape(ep_size, half_slots, model_width),
                "ep",
                split_axis=0,
                concat_axis=0,
                tiled=True,
            )
        )
    returned = jnp.stack(results, axis=1)
    gathered = returned.reshape(experts * capacity, model_width)[position]
    routed = jnp.sum(
        gathered.reshape(tok_rows, top_count, model_width).astype(jnp.float32)
        * route_weights[:, :, None],
        axis=1,
    )
    shared_out = shared_branch(normed, shared_gate, shared_up, shared_down)
    return (routed + shared_out).astype(jnp.bfloat16)


def plan_of(*args):
    peers = lax.axis_size("ep")
    capacity = 3 * args[0].shape[0] * args[2].shape[1] // (2 * peers)
    whole_tiles = capacity % 16 == 0 and peers % 4 == 0 and peers & (peers - 1) == 0
    fits = whole_tiles and lax.axis_size("tp") == 2 and args[4].shape[0] == 1
    return (kernel_body if fits else body)(*args)


def solution(mesh):
    placed = (
        P(("ep", "tp"), None),
        P(),
        P(("ep", "tp"), None),
        P(("ep", "tp"), None),
        P("ep", None, "tp"),
        P("ep", None, "tp"),
        P("ep", "tp", None),
        P(None, "tp"),
        P(None, "tp"),
        P("tp", None),
    )
    return jax.shard_map(
        plan_of, mesh=mesh, in_specs=placed, out_specs=P(("ep", "tp"), None), check_vma=False
    )
```

```python
import functools

import jax
import jax.numpy as jnp
from jax import lax
from jax.experimental import pallas as pl
from jax.experimental.pallas import tpu as pltpu
from jax.sharding import PartitionSpec as P

epsilon = 1e-06
MESH = pl.DeviceIdType.MESH


def toggled(index, step, size):
    total, bit = 0, 1
    while bit < size:
        total = total + bit * ((index // bit + step // bit) % 2)
        bit *= 2
    return total


def gated_sum(rows, gate_w, up_w, down_w):
    total = None
    for half in range(gate_w.shape[0]):
        gate_value = jnp.dot(rows, gate_w[half], preferred_element_type=jnp.float32)
        up_value = jnp.dot(rows, up_w[half], preferred_element_type=jnp.float32)
        hidden = (gate_value / (1.0 + jnp.exp(-gate_value)) * up_value).astype(jnp.bfloat16)
        term = jnp.dot(hidden, down_w[half], preferred_element_type=jnp.float32)
        total = term if total is None else total + term
    return total


def slot_rows(meta, me, steps):
    count = meta.shape[1]
    relative = meta[0:2, :].astype(jnp.int32) ^ me
    step_of = lax.broadcasted_iota(jnp.int32, (steps, count), 0)
    named = (step_of == relative[0:1, :]) | (step_of == relative[1:2, :])
    row_at = lax.broadcasted_iota(jnp.int32, (count, count), 0)
    col_at = lax.broadcasted_iota(jnp.int32, (count, count), 1)
    before = jnp.where(row_at < col_at, 1.0, 0.0).astype(jnp.bfloat16)
    slots = jnp.dot(
        jnp.where(named, 1.0, 0.0).astype(jnp.bfloat16), before, preferred_element_type=jnp.float32
    ).astype(jnp.int32)
    return jnp.where(named, slots, -1)


def picks(slots, steps, capacity):
    slot_at = lax.broadcasted_iota(jnp.int32, (capacity, slots.shape[1]), 0)
    return jnp.concatenate(
        [
            jnp.where(slot_at == slots[step : step + 1, :], 1.0, 0.0).astype(jnp.bfloat16)
            for step in steps
        ],
        axis=0,
    )


def slot_places(meta, me, capacity):
    count = meta.shape[1]
    turned = jnp.transpose(meta)
    relative = turned[:, 0:2].astype(jnp.int32) ^ me
    expert_at = lax.broadcasted_iota(jnp.int32, (count, 128), 1)
    row_at = lax.broadcasted_iota(jnp.int32, (count, count), 0)
    col_at = lax.broadcasted_iota(jnp.int32, (count, count), 1)
    chosen = [expert_at == relative[:, j : j + 1] for j in range(2)]
    after = jnp.where(row_at > col_at, 1.0, 0.0).astype(jnp.bfloat16)
    counted = jnp.dot(
        after,
        jnp.where(chosen[0] | chosen[1], 1.0, 0.0).astype(jnp.bfloat16),
        preferred_element_type=jnp.float32,
    )
    places = [
        relative[:, j : j + 1] * capacity
        + jnp.sum(jnp.where(chosen[j], counted, 0.0), axis=1, keepdims=True).astype(jnp.int32)
        for j in range(2)
    ]
    return places, [turned[:, 2 + j : 3 + j] for j in range(2)]


def weight_matrix(places, weights, first, amount):
    at = lax.broadcasted_iota(jnp.int32, (places[0].shape[0], amount), 1) + first
    scale = jnp.where(at == places[0], weights[0], 0.0) + jnp.where(
        at == places[1], weights[1], 0.0
    )
    upper = scale.astype(jnp.bfloat16)
    return upper, (scale - upper.astype(jnp.float32)).astype(jnp.bfloat16)


def weighted(pair, block):
    return jnp.dot(pair[0], block, preferred_element_type=jnp.float32) + jnp.dot(
        pair[1], block, preferred_element_type=jnp.float32
    )


PIECES = 8
VMEM_MIB = 60
CUTS = 8
OWN_FIRST = 2
ORDER = (
    "2.0", "2.1", "2.2", "2.3", "0.0", "0.1", "S", "2.4", "2.5", "0.2", "0.3", "2.6", "2.7", "A",
    "0.4", "0.5", "B", "0.6", "0.7", "1.0", "1.1", "F.0", "W.0", "P.0", "1.2", "1.3", "P.2", "1.4",
    "1.5", "m", "Y.0", "Y.1", "1.6", "1.7", "Y.2", "Y.3", "F.1", "W.1", "a", "h", "W.2", "Y.4",
    "Y.5", "Y.6", "Y.7", "P.1", "V.0", "V.1", "V.2", "V.3", "V.4", "V.5", "X.0", "X.1", "X.2",
    "X.3", "V.6", "V.7", "X.4", "X.5", "X.6", "X.7", "N", "M",
)


def layer_kernel(
    peers,
    capacity,
    pieces,
    cuts,
    tokens,
    gain,
    expert_ids,
    route_weights,
    expert_gate,
    expert_up,
    expert_down,
    shared_gate,
    shared_up,
    shared_down,
    held,
    sums_in,
    gate_all,
    up_all,
    down_all,
    s_gate_all,
    s_up_all,
    s_down_all,
    raw,
    normed,
    meta,
    outgoing,
    near_in,
    far_in,
    near_out,
    far_out,
    returned,
    total,
    relay_in,
    meta_in,
    picked,
    scales_of,
    relay_out,
    relay_back,
    sums_out,
    pass_in,
    pass_out,
    around,
    token_sems,
    weight_local,
    weight_send,
    weight_recv,
    out_send,
    out_recv,
    back_send,
    back_recv,
    block_send,
    block_recv,
    meta_send,
    meta_recv,
    relay_send,
    relay_recv,
    home_send,
    home_recv,
    sums_send,
    sums_recv,
    pass_send,
    pass_recv,
    middle_send,
    middle_recv,
    side_send,
    side_recv,
    up_send,
    held_send,
):
    me = lax.axis_index("ep")
    core = lax.axis_index("tp")
    sibling = 1 - core
    tok_rows, width = normed.shape
    piece, cut = width // pieces, width // cuts
    half, quarter = peers // 2, peers // 4
    inner = ((me // quarter + 1) // 2) % 2
    far_turn, next_turn = half + quarter, quarter
    turns = (half, half + quarter, quarter)

    def at_step(step):
        return (toggled(me, step, peers), core)

    def columns(c):
        return pl.ds(c * piece, piece)

    def cut_columns(c):
        return pl.ds(c * cut, cut)

    def left(source, sem):
        remote(source, source, sem, sem, at_step(1)).wait_send()

    def landed(target, sem):
        remote(target, target, sem, sem, at_step(1)).wait_recv()

    def on_inner(action):
        pl.when(inner == 1)(action)

    def on_outer(action):
        pl.when(inner == 0)(action)

    def remote(source, target, send, recv, place):
        return pltpu.make_async_remote_copy(
            src_ref=source,
            dst_ref=target,
            send_sem=send,
            recv_sem=recv,
            device_id=place,
            device_id_type=MESH,
        )

    barrier = pltpu.get_barrier_semaphore()
    greeted = [step for step in range(1, half)] + [half, far_turn]
    pl.semaphore_signal(barrier, inc=1, device_id=(me, sibling), device_id_type=MESH)
    for step in greeted:
        pl.semaphore_signal(barrier, inc=1, device_id=at_step(step), device_id_type=MESH)
    bands = token_sems.shape[0]
    band = tok_rows // bands
    fetched = [
        pltpu.make_async_copy(
            tokens.at[pl.ds(i * band, band)], raw.at[pl.ds(i * band, band)], token_sems.at[i]
        )
        for i in range(bands)
    ]
    for copy in fetched:
        copy.start()
    sources = (
        (shared_gate, s_gate_all),
        (shared_up, s_up_all),
        (shared_down, s_down_all),
        (expert_gate, gate_all),
        (expert_up, up_all),
        (expert_down, down_all),
    )
    local = [
        pltpu.make_async_copy(source, target.at[core], weight_local.at[i])
        for i, (source, target) in enumerate(sources)
    ]
    swaps = [
        remote(source, target.at[core], weight_send.at[i], weight_recv.at[i], (me, sibling))
        for i, (source, target) in enumerate(sources)
    ]

    def normalize_rows():
        for i in range(bands):
            fetched[i].wait()
            at = pl.ds(i * band, band)
            values = raw[at].astype(jnp.float32)
            factor = lax.rsqrt(jnp.mean(values * values, axis=1, keepdims=True) + epsilon)
            normed[at] = (values * factor * gain[...]).astype(jnp.bfloat16)

    with jax.named_scope("norm"):
        normalize_rows()
    meta[0:2] = expert_ids[...].astype(jnp.float32)
    meta[2:4] = route_weights[...]
    meta[4:8] = jnp.zeros((4, tok_rows), jnp.float32)

    def meta_copy(side):
        step = {0: half, 1: far_turn, 2: next_turn}[side]
        number = 1 if side == 0 else 0
        return remote(
            meta, meta_in.at[side], meta_send.at[number], meta_recv.at[side], at_step(step)
        )

    def block_copy(side, c):
        return remote(
            normed.at[:, columns(c)],
            relay_in.at[side, :, columns(c)],
            block_send.at[0],
            block_recv.at[side, c],
            at_step(far_turn if side == 1 else next_turn),
        )

    def forward(c):
        return remote(
            relay_in.at[2, :, columns(c)],
            relay_in.at[0, :, columns(c)],
            block_send.at[1],
            block_recv.at[0, c],
            at_step(far_turn),
        )

    def dispatch(step):
        group = step // quarter
        return remote(
            outgoing.at[step],
            near_in.at[step],
            out_send.at[group],
            out_recv.at[group],
            at_step(step),
        )

    def give_back(step):
        return remote(
            near_out.at[step],
            returned.at[step],
            back_send.at[0],
            back_recv.at[0],
            at_step(step),
        )

    def relay(side, k, c):
        target = near_in.at[k + quarter] if side == 2 else far_in.at[side, k % quarter]
        return remote(
            relay_out.at[side, k, :, columns(c)],
            target.at[:, columns(c)],
            relay_send.at[side],
            relay_recv.at[side],
            at_step(k),
        )

    def home(side, j, c):
        k = j + quarter * (1 - inner)
        return remote(
            far_out.at[side, j, :, cut_columns(c)],
            relay_back.at[side, k, :, cut_columns(c)],
            home_send.at[side],
            home_recv.at[side, c],
            at_step(k),
        )

    def sideways(side, j, c):
        source = near_out.at[quarter + j] if side == 2 else far_out.at[side, j]
        return remote(
            source.at[:, cut_columns(c)],
            around.at[side, j, :, cut_columns(c)],
            side_send.at[side],
            side_recv.at[side, c],
            at_step(j),
        )

    def upward(side, j, c):
        if side == 2:
            target, recv = returned.at[quarter + j], back_recv.at[1]
        else:
            target, recv = relay_back.at[side, quarter + j], home_recv.at[side, c]
        return remote(
            around.at[side, j, :, cut_columns(c)],
            target.at[:, cut_columns(c)],
            up_send.at[side],
            recv,
            at_step(next_turn),
        )

    def straight(c):
        return remote(
            near_out.at[quarter, :, cut_columns(c)],
            returned.at[quarter, :, cut_columns(c)],
            up_send.at[3],
            back_recv.at[1],
            at_step(next_turn),
        )

    def middle(j):
        return remote(
            near_out.at[quarter + j],
            relay_back.at[2, j],
            middle_send.at[0],
            middle_recv.at[0],
            at_step(j),
        )

    def sums(side, c):
        target = pass_in if side == 0 else sums_in
        return remote(
            sums_out.at[side, :, cut_columns(c)],
            target.at[:, cut_columns(c)],
            sums_send.at[side],
            pass_recv.at[c] if side == 0 else sums_recv.at[c],
            at_step(far_turn),
        )

    def sums_on(c):
        return remote(
            pass_out.at[:, cut_columns(c)],
            sums_in.at[:, cut_columns(c)],
            pass_send.at[0],
            sums_recv.at[c],
            at_step(next_turn),
        )

    with jax.named_scope("meet"):
        pl.semaphore_wait(barrier, len(greeted) + 1)

    @pl.when(inner == 1)
    def _():
        meta_copy(1).start()
        for c in range(OWN_FIRST):
            block_copy(1, c).start()

    @pl.when(inner == 0)
    def _():
        meta_copy(2).start()
        meta_copy(0).start()
        for c in range(pieces):
            block_copy(2, c).start()

    for copy in local:
        copy.start()
    slots = slot_rows(meta[...], me, half)

    def send_slots(first):
        rows = jnp.dot(
            picks(slots, range(first, first + quarter), capacity),
            normed[...],
            preferred_element_type=jnp.float32,
        ).astype(jnp.bfloat16)
        for i in range(quarter):
            block = rows[i * capacity : (i + 1) * capacity]
            if first + i == 0:
                near_in[0] = block
            else:
                outgoing[first + i] = block
                dispatch(first + i).start()

    on_inner(lambda: send_slots(quarter))
    send_slots(0)
    for copy in swaps:
        copy.start()

    def open_side(side):
        landed(meta_in.at[side], meta_recv.at[side])
        reach = quarter if side == 2 else half
        picked[side, : reach * capacity] = picks(
            slot_rows(meta_in[side], me, half), range(reach), capacity
        )

    def pass_on(side, c):
        if c == 0:
            open_side(side)
        reach = quarter if side == 2 else half
        landed(relay_in.at[side, :, columns(c)], block_recv.at[side, c])
        if side == 2:
            forward(c).start()
            if c == pieces - 1:
                for own in range(OWN_FIRST, pieces):
                    block_copy(1, own).start()
        rows = jnp.dot(
            picked[side, : reach * capacity],
            relay_in[side, :, columns(c)],
            preferred_element_type=jnp.float32,
        ).astype(jnp.bfloat16)
        if side == 2:
            near_in[quarter, :, columns(c)] = rows[:capacity]
        else:
            far_in[side, 0, :, columns(c)] = rows[:capacity]
        for k in range(reach - 1, 0, -1):
            relay_out[side, k, :, columns(c)] = rows[k * capacity : (k + 1) * capacity]
            relay(side, k, c).start()

    def near(group):
        steps = range(group * quarter, (group + 1) * quarter)
        if group == 0:
            landed(near_in.at[pl.ds(1, quarter - 1)], out_recv.at[0])
        else:
            on_outer(lambda: landed(near_in.at[pl.ds(quarter, quarter)], out_recv.at[1]))
            on_inner(
                lambda: landed(near_in.at[pl.ds(quarter + 1, quarter - 1)], relay_recv.at[2])
            )

        block = near_in[group * quarter : (group + 1) * quarter].reshape(quarter * capacity, width)
        out = gated_sum(block, gate_all, up_all, down_all).astype(jnp.bfloat16)
        for i, step in enumerate(steps):
            part = out[i * capacity : (i + 1) * capacity]
            if step == 0:
                returned[0] = part
            else:
                near_out[step] = part

    def near_send():
        for step in range(1, quarter):
            give_back(step).start()

    def middle_send_all():
        relay_back[2, 0] = near_out[quarter]
        for j in range(1, quarter):
            middle(j).start()

    def near_sideways():
        for c in range(cuts):
            straight(c).start()
            for j in range(1, quarter):
                sideways(2, j, c).start()

    def pass_up(side):
        for c in range(cuts):
            with jax.named_scope("up_" + str(c)):
                gathered = around.at[side, pl.ds(1, quarter - 1), :, cut_columns(c)]
                landed(gathered, side_recv.at[side, c])
                for j in range(1, quarter):
                    upward(side, j, c).start()

    def far(side):
        on_outer(lambda: landed(far_in.at[side], relay_recv.at[side]))
        on_inner(lambda: landed(far_in.at[side, pl.ds(1, quarter - 1)], relay_recv.at[side]))
        block = far_in[side].reshape(quarter * capacity, width)
        out = gated_sum(block, gate_all, up_all, down_all).astype(jnp.bfloat16)
        far_out[side] = out.reshape(quarter, capacity, width)

        @pl.when(inner == 1)
        def _():
            relay_back[side, 0] = far_out[side, 0]
            for c in range(cuts):
                for j in range(quarter - 1, 0, -1):
                    home(side, j, c).start()

        @pl.when(inner == 0)
        def _():
            for c in range(cuts):
                for j in range(1, quarter):
                    sideways(side, j, c).start()
                home(side, 0, c).start()

    def prepare(side, source, reach):
        places, scales = slot_places(source[...], me, capacity)
        upper, lower = weight_matrix(places, scales, 0, reach * capacity)
        scales_of[side, 0, :, : reach * capacity] = upper
        scales_of[side, 1, :, : reach * capacity] = lower

    def weighted_by(side, reach, block):
        span = reach * capacity
        pair = (scales_of[side, 0, :, :span], scales_of[side, 1, :, :span])
        return weighted(pair, block.reshape(span, block.shape[-1]))

    def send_sums(side, c):
        landed(relay_back.at[side, pl.ds(1, half - 1), :, cut_columns(c)], home_recv.at[side, c])
        block = relay_back[side, :, :, cut_columns(c)]
        sums_out[side, :, cut_columns(c)] = weighted_by(side, half, block).astype(jnp.bfloat16)
        sums(side, c).start()

    def send_on(c):
        if c == 0:
            landed(relay_back.at[2, pl.ds(1, quarter - 1)], middle_recv.at[0])
        block = relay_back[2, :quarter, :, cut_columns(c)]
        own = weighted_by(2, quarter, block)
        at = cut_columns(c)
        landed(pass_in.at[:, at], pass_recv.at[c])
        pass_out[:, at] = (own + pass_in[:, at].astype(jnp.float32)).astype(jnp.bfloat16)
        sums_on(c).start()

    def shared():
        for i in range(len(sources)):
            local[i].wait()
            swaps[i].wait()
        total[...] = gated_sum(normed[...], s_gate_all, s_up_all, s_down_all)

    def near_total():
        prepare(3, meta, half)
        landed(returned.at[pl.ds(1, quarter - 1)], back_recv.at[0])
        total[...] += weighted_by(3, quarter, returned[:quarter])

    def outer_total():
        span = quarter * capacity
        landed(returned.at[pl.ds(quarter, quarter)], back_recv.at[1])
        pair = (scales_of[3, 0, :, span:], scales_of[3, 1, :, span:])
        total[...] += weighted(pair, returned[quarter:].reshape(span, width))

    actions = {
        "S": shared,
        "A": lambda: near(0),
        "B": lambda: near(1),
        "a": near_send,
        "m": lambda: on_inner(middle_send_all),
        "h": lambda: on_outer(near_sideways),
        "N": near_total,
        "M": lambda: on_inner(outer_total),
    }
    numbered = {
        "0": lambda c: on_inner(lambda: pass_on(0, c)),
        "1": lambda c: on_inner(lambda: pass_on(1, c)),
        "2": lambda c: on_inner(lambda: pass_on(2, c)),
        "F": far,
        "W": lambda side: on_outer(lambda: pass_up(side)),
        "P": lambda side: on_inner(
            lambda: prepare(side, meta_in.at[side], quarter if side == 2 else half)
        ),
        "V": lambda c: on_inner(lambda: send_on(c)),
        "X": lambda c: on_inner(lambda: send_sums(1, c)),
        "Y": lambda c: on_inner(lambda: send_sums(0, c)),
    }
    for name in ORDER:
        with jax.named_scope("do_" + name):
            if name in actions:
                actions[name]()
            else:
                numbered[name[0]](int(name[2:]))

    keep = pltpu.make_async_copy(total, held, held_send.at[0])
    keep.start()
    with jax.named_scope("settle"):
        left(outgoing.at[pl.ds(1, quarter - 1)], out_send.at[0])
        left(near_out.at[pl.ds(1, quarter - 1)], back_send.at[0])
        left(normed, block_send.at[0])

        @pl.when(inner == 0)
        def _():
            left(meta, meta_send.at[0])
            left(meta, meta_send.at[1])
            left(near_out.at[quarter], up_send.at[3])
            for side in range(2):
                left(far_out.at[side, 0], home_send.at[side])
            for side in range(3):
                left(around.at[side, pl.ds(1, quarter - 1)], side_send.at[side])
                left(around.at[side, pl.ds(1, quarter - 1)], up_send.at[side])

        @pl.when(inner == 1)
        def _():
            left(meta, meta_send.at[0])
            left(outgoing.at[pl.ds(quarter, quarter)], out_send.at[1])
            left(near_out.at[pl.ds(1, quarter - 1)], middle_send.at[0])
            left(normed, block_send.at[1])
            for side in range(2):
                left(far_out.at[side, pl.ds(1, quarter - 1)], home_send.at[side])
                left(relay_out.at[side, pl.ds(1, half - 1)], relay_send.at[side])
                left(normed, sums_send.at[side])
            left(relay_out.at[2, pl.ds(1, quarter - 1)], relay_send.at[2])
            left(normed, pass_send.at[0])

        keep.wait()
        for c in range(cuts):
            landed(sums_in.at[:, cut_columns(c)], sums_recv.at[c])


def kernel_body(
    tokens,
    norm_gain,
    expert_ids,
    route_weights,
    expert_gate,
    expert_up,
    expert_down,
    shared_gate,
    shared_up,
    shared_down,
):
    peers = lax.axis_size("ep")
    halves = lax.axis_size("tp")
    tok_rows, width = tokens.shape
    capacity = 3 * tok_rows * expert_ids.shape[1] // (2 * peers)
    half, quarter, pieces, cuts, bands = peers // 2, peers // 4, PIECES, CUTS, 4
    vmem = pl.BlockSpec(memory_space=pltpu.VMEM)
    anywhere = pl.BlockSpec(memory_space=pl.ANY)
    weights = (
        expert_gate[0],
        expert_up[0],
        expert_down[0],
        shared_gate,
        shared_up,
        shared_down,
    )

    def rows(*shape):
        return pltpu.VMEM(shape, jnp.bfloat16)

    dma = pltpu.SemaphoreType.DMA
    held, arrived = pl.pallas_call(
        functools.partial(layer_kernel, peers, capacity, pieces, cuts),
        out_shape=[
            jax.ShapeDtypeStruct((tok_rows, width), jnp.float32),
            jax.ShapeDtypeStruct((tok_rows, width), jnp.bfloat16),
        ],
        in_specs=[anywhere] + [vmem] * 3 + [anywhere] * 6,
        out_specs=[anywhere] * 2,
        scratch_shapes=[pltpu.VMEM((halves,) + w.shape, w.dtype) for w in weights]
        + [
            rows(tok_rows, width),
            rows(tok_rows, width),
            pltpu.VMEM((8, tok_rows), jnp.float32),
            rows(half, capacity, width),
            rows(half, capacity, width),
            rows(2, quarter, capacity, width),
            rows(half, capacity, width),
            rows(2, quarter, capacity, width),
            rows(half, capacity, width),
            pltpu.VMEM((tok_rows, width), jnp.float32),
            rows(3, tok_rows, width),
            pltpu.VMEM((3, 8, tok_rows), jnp.float32),
            rows(3, half * capacity, tok_rows),
            rows(4, 2, tok_rows, half * capacity),
            rows(3, half, capacity, width),
            rows(3, half, capacity, width),
            rows(2, tok_rows, width),
            rows(tok_rows, width),
            rows(tok_rows, width),
            rows(3, quarter, capacity, width),
        ]
        + [dma((bands,))]
        + [dma((len(weights),))] * 3
        + [dma((2,)), dma((2,)), dma((1,)), dma((2,))]
        + [dma((2,)), dma((3, pieces)), dma((2,)), dma((3,))]
        + [dma((3,)), dma((3,)), dma((2,)), dma((2, cuts))]
        + [dma((2,)), dma((cuts,)), dma((1,)), dma((cuts,)), dma((1,)), dma((1,))]
        + [dma((3,)), dma((3, cuts)), dma((4,)), dma((1,))],
        compiler_params=pltpu.CompilerParams(
            collective_id=0, has_side_effects=True, vmem_limit_bytes=VMEM_MIB * 1024 * 1024
        ),
        name="layer",
    )(tokens, norm_gain.reshape(1, width), expert_ids.T, route_weights.T, *weights)
    return (held + arrived.astype(jnp.float32)).astype(jnp.bfloat16)


def normalize(tokens, norm_gain):
    values = tokens.astype(jnp.float32)
    factor = lax.rsqrt(jnp.mean(values * values, axis=1, keepdims=True) + epsilon)
    return (values * factor * norm_gain[None, :]).astype(jnp.bfloat16)


def round_term(partial_value):
    return lax.optimization_barrier(partial_value.astype(jnp.bfloat16)).astype(jnp.float32)


def gated_rows(row_block, gate_w, up_w):
    gate_value = jnp.dot(row_block, gate_w, preferred_element_type=jnp.float32)
    up_value = jnp.dot(row_block, up_w, preferred_element_type=jnp.float32)
    return (jax.nn.silu(gate_value) * up_value).astype(jnp.bfloat16)


def sliced_term(hidden, down_w):
    return round_term(jnp.dot(hidden, down_w, preferred_element_type=jnp.float32))


def shared_branch(normed, shared_gate, shared_up, shared_down):
    hidden = gated_rows(lax.all_gather(normed, "tp", axis=0, tiled=True), shared_gate, shared_up)
    return lax.psum_scatter(
        sliced_term(hidden, shared_down).astype(jnp.bfloat16), "tp", scatter_dimension=0, tiled=True
    ).astype(jnp.float32)


def body(
    tokens,
    norm_gain,
    expert_ids,
    route_weights,
    expert_gate,
    expert_up,
    expert_down,
    shared_gate,
    shared_up,
    shared_down,
):
    normed = normalize(tokens, norm_gain)
    tok_rows = tokens.shape[0]
    model_width = tokens.shape[1]
    top_count = expert_ids.shape[1]
    ep_size = lax.axis_size("ep")
    experts = expert_gate.shape[0] * ep_size
    capacity = 3 * tok_rows * top_count // (2 * experts)
    assigned = tok_rows * top_count
    gate_one = expert_gate[0]
    up_one = expert_up[0]
    down_one = expert_down[0]
    flat_ids = expert_ids.reshape(-1)
    onehot = (flat_ids[:, None] == jnp.arange(experts, dtype=jnp.int32)[None, :]).astype(
        jnp.bfloat16
    )
    earlier = (jnp.arange(assigned)[:, None] > jnp.arange(assigned)[None, :]).astype(jnp.bfloat16)
    before_count = jnp.dot(earlier, onehot, preferred_element_type=jnp.float32)
    slot_index = jnp.sum(before_count * onehot.astype(jnp.float32), axis=1).astype(jnp.int32)
    position = flat_ids * capacity + slot_index
    owners = (
        jnp.full((experts * capacity,), tok_rows, jnp.int32)
        .at[position]
        .set(jnp.arange(assigned, dtype=jnp.int32) // top_count)
    )
    padded = jnp.concatenate([normed, jnp.zeros((1, model_width), jnp.bfloat16)], axis=0)
    outgoing = padded[owners].reshape(ep_size, capacity, model_width)
    half_slots = capacity // 2
    split_rows = outgoing.reshape(ep_size, 2, half_slots, model_width)
    results = []
    for portion in range(2):
        received = lax.all_to_all(
            split_rows[:, portion], "ep", split_axis=0, concat_axis=0, tiled=True
        )
        hidden = gated_rows(
            lax.all_gather(
                received.reshape(ep_size * half_slots, model_width), "tp", axis=0, tiled=True
            ),
            gate_one,
            up_one,
        )
        summed = lax.psum_scatter(
            sliced_term(hidden, down_one).astype(jnp.bfloat16),
            "tp",
            scatter_dimension=0,
            tiled=True,
        )
        results.append(
            lax.all_to_all(
                summed.reshape(ep_size, half_slots, model_width),
                "ep",
                split_axis=0,
                concat_axis=0,
                tiled=True,
            )
        )
    returned = jnp.stack(results, axis=1)
    gathered = returned.reshape(experts * capacity, model_width)[position]
    routed = jnp.sum(
        gathered.reshape(tok_rows, top_count, model_width).astype(jnp.float32)
        * route_weights[:, :, None],
        axis=1,
    )
    shared_out = shared_branch(normed, shared_gate, shared_up, shared_down)
    return (routed + shared_out).astype(jnp.bfloat16)


def plan_of(*args):
    peers = lax.axis_size("ep")
    capacity = 3 * args[0].shape[0] * args[2].shape[1] // (2 * peers)
    whole_tiles = capacity % 16 == 0 and peers % 4 == 0 and peers & (peers - 1) == 0
    fits = whole_tiles and lax.axis_size("tp") == 2 and args[4].shape[0] == 1
    return (kernel_body if fits else body)(*args)


def solution(mesh):
    placed = (
        P(("ep", "tp"), None),
        P(),
        P(("ep", "tp"), None),
        P(("ep", "tp"), None),
        P("ep", None, "tp"),
        P("ep", None, "tp"),
        P("ep", "tp", None),
        P(None, "tp"),
        P(None, "tp"),
        P("tp", None),
    )
    return jax.shard_map(
        plan_of, mesh=mesh, in_specs=placed, out_specs=P(("ep", "tp"), None), check_vma=False
    )
```

```python
import functools

import jax
import jax.numpy as jnp
from jax import lax
from jax.experimental import pallas as pl
from jax.experimental.pallas import tpu as pltpu
from jax.sharding import PartitionSpec as P

epsilon = 1e-06
MESH = pl.DeviceIdType.MESH


def toggled(index, step, size):
    total, bit = 0, 1
    while bit < size:
        total = total + bit * ((index // bit + step // bit) % 2)
        bit *= 2
    return total


def gated_sum(rows, gate_w, up_w, down_w):
    total = None
    for half in range(gate_w.shape[0]):
        gate_value = jnp.dot(rows, gate_w[half], preferred_element_type=jnp.float32)
        up_value = jnp.dot(rows, up_w[half], preferred_element_type=jnp.float32)
        hidden = (gate_value / (1.0 + jnp.exp(-gate_value)) * up_value).astype(jnp.bfloat16)
        term = jnp.dot(hidden, down_w[half], preferred_element_type=jnp.float32)
        total = term if total is None else total + term
    return total


def slot_rows(meta, me, steps):
    count = meta.shape[1]
    relative = meta[0:2, :].astype(jnp.int32) ^ me
    step_of = lax.broadcasted_iota(jnp.int32, (steps, count), 0)
    named = (step_of == relative[0:1, :]) | (step_of == relative[1:2, :])
    row_at = lax.broadcasted_iota(jnp.int32, (count, count), 0)
    col_at = lax.broadcasted_iota(jnp.int32, (count, count), 1)
    before = jnp.where(row_at < col_at, 1.0, 0.0).astype(jnp.bfloat16)
    slots = jnp.dot(
        jnp.where(named, 1.0, 0.0).astype(jnp.bfloat16), before, preferred_element_type=jnp.float32
    ).astype(jnp.int32)
    return jnp.where(named, slots, -1)


def picks(slots, steps, capacity):
    slot_at = lax.broadcasted_iota(jnp.int32, (capacity, slots.shape[1]), 0)
    return jnp.concatenate(
        [
            jnp.where(slot_at == slots[step : step + 1, :], 1.0, 0.0).astype(jnp.bfloat16)
            for step in steps
        ],
        axis=0,
    )


def slot_places(meta, me, capacity):
    count = meta.shape[1]
    turned = jnp.transpose(meta)
    relative = turned[:, 0:2].astype(jnp.int32) ^ me
    expert_at = lax.broadcasted_iota(jnp.int32, (count, 128), 1)
    row_at = lax.broadcasted_iota(jnp.int32, (count, count), 0)
    col_at = lax.broadcasted_iota(jnp.int32, (count, count), 1)
    chosen = [expert_at == relative[:, j : j + 1] for j in range(2)]
    after = jnp.where(row_at > col_at, 1.0, 0.0).astype(jnp.bfloat16)
    counted = jnp.dot(
        after,
        jnp.where(chosen[0] | chosen[1], 1.0, 0.0).astype(jnp.bfloat16),
        preferred_element_type=jnp.float32,
    )
    places = [
        relative[:, j : j + 1] * capacity
        + jnp.sum(jnp.where(chosen[j], counted, 0.0), axis=1, keepdims=True).astype(jnp.int32)
        for j in range(2)
    ]
    return places, [turned[:, 2 + j : 3 + j] for j in range(2)]


def weight_matrix(places, weights, first, amount):
    at = lax.broadcasted_iota(jnp.int32, (places[0].shape[0], amount), 1) + first
    scale = jnp.where(at == places[0], weights[0], 0.0) + jnp.where(
        at == places[1], weights[1], 0.0
    )
    upper = scale.astype(jnp.bfloat16)
    return upper, (scale - upper.astype(jnp.float32)).astype(jnp.bfloat16)


def weighted(pair, block):
    return jnp.dot(pair[0], block, preferred_element_type=jnp.float32) + jnp.dot(
        pair[1], block, preferred_element_type=jnp.float32
    )


PIECES = 8
VMEM_MIB = 60
CUTS = 8
OWN_FIRST = (2, 2)
ORDER = (
    "2.0", "2.1", "2.2", "2.3", "0.0", "0.1", "2.4", "2.5", "0.2", "0.3", "2.6", "2.7", "Q", "O.1",
    "0.4", "0.5", "S", "0.6", "0.7", "3.0", "3.1", "3.2", "3.3", "F.0", "W.0", "O.0", "3.4", "3.5",
    "A", "B", "P.0", "4.0", "4.1", "P.2", "m", "4.2", "4.3", "h", "3.6", "3.7", "4.4", "4.5",
    "Y.0", "Y.1", "4.6", "4.7", "Y.2", "Y.3", "Y.4", "Y.5", "Y.6", "Y.7", "F.1", "W.1", "W.2", "a",
    "P.1", "V.0", "V.1", "V.2", "V.3", "V.4", "V.5", "X.0", "X.1", "X.2", "X.3", "V.6", "V.7",
    "X.4", "X.5", "X.6", "X.7", "N", "M",
)


def layer_kernel(
    peers,
    capacity,
    pieces,
    cuts,
    tokens,
    gain,
    expert_ids,
    route_weights,
    expert_gate,
    expert_up,
    expert_down,
    shared_gate,
    shared_up,
    shared_down,
    held,
    sums_in,
    gate_all,
    up_all,
    down_all,
    s_gate_all,
    s_up_all,
    s_down_all,
    raw,
    normed,
    meta,
    outgoing,
    near_in,
    far_in,
    near_out,
    far_out,
    returned,
    total,
    relay_in,
    meta_in,
    picked,
    scales_of,
    relay_out,
    relay_back,
    sums_out,
    pass_in,
    pass_out,
    around,
    token_sems,
    weight_local,
    weight_send,
    weight_recv,
    out_send,
    out_recv,
    back_send,
    back_recv,
    block_send,
    block_recv,
    meta_send,
    meta_recv,
    relay_send,
    relay_recv,
    home_send,
    home_recv,
    sums_send,
    sums_recv,
    pass_send,
    pass_recv,
    middle_send,
    middle_recv,
    side_send,
    side_recv,
    up_send,
    held_send,
    turn,
):
    me = lax.axis_index("ep")
    core = lax.axis_index("tp")
    sibling = 1 - core
    tok_rows, width = normed.shape
    piece, cut = width // pieces, width // cuts
    half, quarter = peers // 2, peers // 4
    inner = ((me // quarter + 1) // 2) % 2
    far_turn, next_turn = half + quarter, quarter
    turns = (half, half + quarter, quarter)

    def at_step(step):
        return (toggled(me, step, peers), core)

    def columns(c):
        return pl.ds(c * piece, piece)

    def cut_columns(c):
        return pl.ds(c * cut, cut)

    def left(source, sem):
        remote(source, source, sem, sem, at_step(1)).wait_send()

    def landed(target, sem):
        remote(target, target, sem, sem, at_step(1)).wait_recv()

    def on_inner(action):
        pl.when(inner == 1)(action)

    def on_outer(action):
        pl.when(inner == 0)(action)

    def remote(source, target, send, recv, place):
        return pltpu.make_async_remote_copy(
            src_ref=source,
            dst_ref=target,
            send_sem=send,
            recv_sem=recv,
            device_id=place,
            device_id_type=MESH,
        )

    barrier = pltpu.get_barrier_semaphore()
    greeted = [step for step in range(1, half)] + [half, far_turn]
    pl.semaphore_signal(barrier, inc=1, device_id=(me, sibling), device_id_type=MESH)
    for step in greeted:
        pl.semaphore_signal(barrier, inc=1, device_id=at_step(step), device_id_type=MESH)
    bands = token_sems.shape[0]
    band = tok_rows // bands
    fetched = [
        pltpu.make_async_copy(
            tokens.at[pl.ds(i * band, band)], raw.at[pl.ds(i * band, band)], token_sems.at[i]
        )
        for i in range(bands)
    ]
    for copy in fetched:
        copy.start()
    sources = (
        (shared_gate, s_gate_all),
        (shared_up, s_up_all),
        (shared_down, s_down_all),
        (expert_gate, gate_all),
        (expert_up, up_all),
        (expert_down, down_all),
    )
    local = [
        pltpu.make_async_copy(source, target.at[core], weight_local.at[i])
        for i, (source, target) in enumerate(sources)
    ]
    swaps = [
        remote(source, target.at[core], weight_send.at[i], weight_recv.at[i], (me, sibling))
        for i, (source, target) in enumerate(sources)
    ]

    def normalize_rows():
        for i in range(bands):
            fetched[i].wait()
            at = pl.ds(i * band, band)
            values = raw[at].astype(jnp.float32)
            factor = lax.rsqrt(jnp.mean(values * values, axis=1, keepdims=True) + epsilon)
            normed[at] = (values * factor * gain[...]).astype(jnp.bfloat16)

    with jax.named_scope("norm"):
        normalize_rows()
    meta[0:2] = expert_ids[...].astype(jnp.float32)
    meta[2:4] = route_weights[...]
    meta[4:8] = jnp.zeros((4, tok_rows), jnp.float32)

    def meta_copy(side):
        step = {0: half, 1: far_turn, 2: next_turn}[side]
        number = 1 if side == 0 else 0
        return remote(
            meta, meta_in.at[side], meta_send.at[number], meta_recv.at[side], at_step(step)
        )

    def block_copy(side, c):
        return remote(
            normed.at[:, columns(c)],
            relay_in.at[side, :, columns(c)],
            block_send.at[0],
            block_recv.at[side, c],
            at_step(far_turn if side == 1 else next_turn),
        )

    def forward(c):
        return remote(
            relay_in.at[2, :, columns(c)],
            relay_in.at[0, :, columns(c)],
            block_send.at[1],
            block_recv.at[0, c],
            at_step(far_turn),
        )

    def dispatch(step):
        group = step // quarter
        return remote(
            outgoing.at[step],
            near_in.at[step],
            out_send.at[group],
            out_recv.at[group],
            at_step(step),
        )

    def give_back(step):
        return remote(
            near_out.at[step],
            returned.at[step],
            back_send.at[0],
            back_recv.at[0],
            at_step(step),
        )

    def relay(side, k, c):
        target = near_in.at[k + quarter] if side == 2 else far_in.at[side, k % quarter]
        return remote(
            relay_out.at[side, k, :, columns(c)],
            target.at[:, columns(c)],
            relay_send.at[side],
            relay_recv.at[side],
            at_step(k),
        )

    def home(side, j, c):
        k = j + quarter * (1 - inner)
        return remote(
            far_out.at[side, j, :, cut_columns(c)],
            relay_back.at[side, k, :, cut_columns(c)],
            home_send.at[side],
            home_recv.at[side, c],
            at_step(k),
        )

    def sideways(side, j, c):
        source = near_out.at[quarter + j] if side == 2 else far_out.at[side, j]
        return remote(
            source.at[:, cut_columns(c)],
            around.at[side, j, :, cut_columns(c)],
            side_send.at[side],
            side_recv.at[side, c],
            at_step(j),
        )

    def upward(side, j, c):
        if side == 2:
            target, recv = returned.at[quarter + j], back_recv.at[1]
        else:
            target, recv = relay_back.at[side, quarter + j], home_recv.at[side, c]
        return remote(
            around.at[side, j, :, cut_columns(c)],
            target.at[:, cut_columns(c)],
            up_send.at[side],
            recv,
            at_step(next_turn),
        )

    def straight(c):
        return remote(
            near_out.at[quarter, :, cut_columns(c)],
            returned.at[quarter, :, cut_columns(c)],
            up_send.at[3],
            back_recv.at[1],
            at_step(next_turn),
        )

    def middle(j):
        return remote(
            near_out.at[quarter + j],
            relay_back.at[2, j],
            middle_send.at[0],
            middle_recv.at[0],
            at_step(j),
        )

    def sums(side, c):
        target = pass_in if side == 0 else sums_in
        return remote(
            sums_out.at[side, :, cut_columns(c)],
            target.at[:, cut_columns(c)],
            sums_send.at[side],
            pass_recv.at[c] if side == 0 else sums_recv.at[c],
            at_step(far_turn),
        )

    def sums_on(c):
        return remote(
            pass_out.at[:, cut_columns(c)],
            sums_in.at[:, cut_columns(c)],
            pass_send.at[0],
            sums_recv.at[c],
            at_step(next_turn),
        )

    def start_own(which, first, last):
        if last > first:

            @pl.when(core == which)
            def _():
                for c in range(first, last):
                    block_copy(1, c).start()

    def start_block():
        for c in range(pieces):
            block_copy(2, c).start()

    with jax.named_scope("meet"):
        pl.semaphore_wait(barrier, len(greeted) + 1)

    @pl.when(inner == 1)
    def _():
        meta_copy(1).start()
        start_own(1, 0, OWN_FIRST[1])

    @pl.when(inner == 0)
    def _():
        meta_copy(2).start()
        meta_copy(0).start()
        pl.when(core == 0)(start_block)

    for copy in local:
        copy.start()
    slots = slot_rows(meta[...], me, half)

    def send_slots(first):
        rows = jnp.dot(
            picks(slots, range(first, first + quarter), capacity),
            normed[...],
            preferred_element_type=jnp.float32,
        ).astype(jnp.bfloat16)
        for i in range(quarter):
            block = rows[i * capacity : (i + 1) * capacity]
            if first + i == 0:
                near_in[0] = block
            else:
                outgoing[first + i] = block
                dispatch(first + i).start()

    on_inner(lambda: send_slots(quarter))
    send_slots(0)
    for copy in swaps:
        copy.start()

    @pl.when((inner == 0) & (core == 0))
    def _():
        left(normed, block_send.at[0])
        pl.semaphore_signal(turn, inc=1, device_id=(me, sibling), device_id_type=MESH)

    @pl.when((inner == 0) & (core == 1))
    def _():
        pl.semaphore_wait(turn, 1)
        start_block()

    def open_side(side):
        landed(meta_in.at[side], meta_recv.at[side])
        reach = quarter if side == 2 else half
        picked[side, : reach * capacity] = picks(
            slot_rows(meta_in[side], me, half), range(reach), capacity
        )

    def pass_on(side, c):
        if c == 0:
            open_side(side)
        reach = quarter if side == 2 else half
        landed(relay_in.at[side, :, columns(c)], block_recv.at[side, c])
        if side == 2:
            forward(c).start()
        rows = jnp.dot(
            picked[side, : reach * capacity],
            relay_in[side, :, columns(c)],
            preferred_element_type=jnp.float32,
        ).astype(jnp.bfloat16)
        if side == 2:
            near_in[quarter, :, columns(c)] = rows[:capacity]
        else:
            far_in[side, 0, :, columns(c)] = rows[:capacity]
        for k in range(reach - 1, 0, -1):
            relay_out[side, k, :, columns(c)] = rows[k * capacity : (k + 1) * capacity]
            relay(side, k, c).start()

    def near(group):
        steps = range(group * quarter, (group + 1) * quarter)
        if group == 0:
            landed(near_in.at[pl.ds(1, quarter - 1)], out_recv.at[0])
        else:
            on_outer(lambda: landed(near_in.at[pl.ds(quarter, quarter)], out_recv.at[1]))
            on_inner(
                lambda: landed(near_in.at[pl.ds(quarter + 1, quarter - 1)], relay_recv.at[2])
            )

        block = near_in[group * quarter : (group + 1) * quarter].reshape(quarter * capacity, width)
        out = gated_sum(block, gate_all, up_all, down_all).astype(jnp.bfloat16)
        for i, step in enumerate(steps):
            part = out[i * capacity : (i + 1) * capacity]
            if step == 0:
                returned[0] = part
            else:
                near_out[step] = part

    def near_send():
        for step in range(1, quarter):
            give_back(step).start()

    def middle_send_all():
        relay_back[2, 0] = near_out[quarter]
        for j in range(1, quarter):
            middle(j).start()

    def near_sideways():
        for c in range(cuts):
            straight(c).start()
            for j in range(1, quarter):
                sideways(2, j, c).start()

    def pass_up(side):
        for c in range(cuts):
            with jax.named_scope("up_" + str(c)):
                gathered = around.at[side, pl.ds(1, quarter - 1), :, cut_columns(c)]
                landed(gathered, side_recv.at[side, c])
                for j in range(1, quarter):
                    upward(side, j, c).start()

    def far(side):
        on_outer(lambda: landed(far_in.at[side], relay_recv.at[side]))
        on_inner(lambda: landed(far_in.at[side, pl.ds(1, quarter - 1)], relay_recv.at[side]))
        block = far_in[side].reshape(quarter * capacity, width)
        out = gated_sum(block, gate_all, up_all, down_all).astype(jnp.bfloat16)
        far_out[side] = out.reshape(quarter, capacity, width)

        @pl.when(inner == 1)
        def _():
            relay_back[side, 0] = far_out[side, 0]
            for c in range(cuts):
                for j in range(quarter - 1, 0, -1):
                    home(side, j, c).start()

        @pl.when(inner == 0)
        def _():
            for c in range(cuts):
                for j in range(1, quarter):
                    sideways(side, j, c).start()
                home(side, 0, c).start()

    def prepare(side, source, reach):
        places, scales = slot_places(source[...], me, capacity)
        upper, lower = weight_matrix(places, scales, 0, reach * capacity)
        scales_of[side, 0, :, : reach * capacity] = upper
        scales_of[side, 1, :, : reach * capacity] = lower

    def weighted_by(side, reach, block):
        span = reach * capacity
        pair = (scales_of[side, 0, :, :span], scales_of[side, 1, :, :span])
        return weighted(pair, block.reshape(span, block.shape[-1]))

    def send_sums(side, c):
        landed(relay_back.at[side, pl.ds(1, half - 1), :, cut_columns(c)], home_recv.at[side, c])
        block = relay_back[side, :, :, cut_columns(c)]
        sums_out[side, :, cut_columns(c)] = weighted_by(side, half, block).astype(jnp.bfloat16)
        sums(side, c).start()

    def send_on(c):
        if c == 0:
            landed(relay_back.at[2, pl.ds(1, quarter - 1)], middle_recv.at[0])
        block = relay_back[2, :quarter, :, cut_columns(c)]
        own = weighted_by(2, quarter, block)
        at = cut_columns(c)
        landed(pass_in.at[:, at], pass_recv.at[c])
        pass_out[:, at] = (own + pass_in[:, at].astype(jnp.float32)).astype(jnp.bfloat16)
        sums_on(c).start()

    def shared():
        for i in range(len(sources)):
            local[i].wait()
            swaps[i].wait()
        total[...] = gated_sum(normed[...], s_gate_all, s_up_all, s_down_all)

    def near_total():
        prepare(3, meta, half)
        landed(returned.at[pl.ds(1, quarter - 1)], back_recv.at[0])
        total[...] += weighted_by(3, quarter, returned[:quarter])

    def outer_total():
        span = quarter * capacity
        landed(returned.at[pl.ds(quarter, quarter)], back_recv.at[1])
        pair = (scales_of[3, 0, :, span:], scales_of[3, 1, :, span:])
        total[...] += weighted(pair, returned[quarter:].reshape(span, width))

    actions = {
        "S": shared,
        "A": lambda: near(0),
        "B": lambda: near(1),
        "a": near_send,
        "m": lambda: on_inner(middle_send_all),
        "h": lambda: on_outer(near_sideways),
        "N": near_total,
        "Q": lambda: on_inner(lambda: start_own(0, 0, OWN_FIRST[0])),
        "M": lambda: on_inner(outer_total),
    }
    numbered = {
        "0": lambda c: on_inner(lambda: pass_on(0, c)),
        "1": lambda c: on_inner(lambda: pass_on(1, c)),
        "2": lambda c: on_inner(lambda: pass_on(2, c)),
        "3": lambda c: pl.when((inner == 1) & (core == 1))(lambda: pass_on(1, c)),
        "4": lambda c: pl.when((inner == 1) & (core == 0))(lambda: pass_on(1, c)),
        "O": lambda which: on_inner(lambda: start_own(which, OWN_FIRST[which], pieces)),
        "F": far,
        "W": lambda side: on_outer(lambda: pass_up(side)),
        "P": lambda side: on_inner(
            lambda: prepare(side, meta_in.at[side], quarter if side == 2 else half)
        ),
        "V": lambda c: on_inner(lambda: send_on(c)),
        "X": lambda c: on_inner(lambda: send_sums(1, c)),
        "Y": lambda c: on_inner(lambda: send_sums(0, c)),
    }
    for name in ORDER:
        with jax.named_scope("do_" + name):
            if name in actions:
                actions[name]()
            else:
                numbered[name[0]](int(name[2:]))

    keep = pltpu.make_async_copy(total, held, held_send.at[0])
    keep.start()
    with jax.named_scope("settle"):
        left(outgoing.at[pl.ds(1, quarter - 1)], out_send.at[0])
        left(near_out.at[pl.ds(1, quarter - 1)], back_send.at[0])

        @pl.when((inner == 1) | (core == 1))
        def _():
            left(normed, block_send.at[0])

        @pl.when(inner == 0)
        def _():
            left(meta, meta_send.at[0])
            left(meta, meta_send.at[1])
            left(near_out.at[quarter], up_send.at[3])
            for side in range(2):
                left(far_out.at[side, 0], home_send.at[side])
            for side in range(3):
                left(around.at[side, pl.ds(1, quarter - 1)], side_send.at[side])
                left(around.at[side, pl.ds(1, quarter - 1)], up_send.at[side])

        @pl.when(inner == 1)
        def _():
            left(meta, meta_send.at[0])
            left(outgoing.at[pl.ds(quarter, quarter)], out_send.at[1])
            left(near_out.at[pl.ds(1, quarter - 1)], middle_send.at[0])
            left(normed, block_send.at[1])
            for side in range(2):
                left(far_out.at[side, pl.ds(1, quarter - 1)], home_send.at[side])
                left(relay_out.at[side, pl.ds(1, half - 1)], relay_send.at[side])
                left(normed, sums_send.at[side])
            left(relay_out.at[2, pl.ds(1, quarter - 1)], relay_send.at[2])
            left(normed, pass_send.at[0])

        keep.wait()
        for c in range(cuts):
            landed(sums_in.at[:, cut_columns(c)], sums_recv.at[c])


def kernel_body(
    tokens,
    norm_gain,
    expert_ids,
    route_weights,
    expert_gate,
    expert_up,
    expert_down,
    shared_gate,
    shared_up,
    shared_down,
):
    peers = lax.axis_size("ep")
    halves = lax.axis_size("tp")
    tok_rows, width = tokens.shape
    capacity = 3 * tok_rows * expert_ids.shape[1] // (2 * peers)
    half, quarter, pieces, cuts, bands = peers // 2, peers // 4, PIECES, CUTS, 4
    vmem = pl.BlockSpec(memory_space=pltpu.VMEM)
    anywhere = pl.BlockSpec(memory_space=pl.ANY)
    weights = (
        expert_gate[0],
        expert_up[0],
        expert_down[0],
        shared_gate,
        shared_up,
        shared_down,
    )

    def rows(*shape):
        return pltpu.VMEM(shape, jnp.bfloat16)

    dma = pltpu.SemaphoreType.DMA
    held, arrived = pl.pallas_call(
        functools.partial(layer_kernel, peers, capacity, pieces, cuts),
        out_shape=[
            jax.ShapeDtypeStruct((tok_rows, width), jnp.float32),
            jax.ShapeDtypeStruct((tok_rows, width), jnp.bfloat16),
        ],
        in_specs=[anywhere] + [vmem] * 3 + [anywhere] * 6,
        out_specs=[anywhere] * 2,
        scratch_shapes=[pltpu.VMEM((halves,) + w.shape, w.dtype) for w in weights]
        + [
            rows(tok_rows, width),
            rows(tok_rows, width),
            pltpu.VMEM((8, tok_rows), jnp.float32),
            rows(half, capacity, width),
            rows(half, capacity, width),
            rows(2, quarter, capacity, width),
            rows(half, capacity, width),
            rows(2, quarter, capacity, width),
            rows(half, capacity, width),
            pltpu.VMEM((tok_rows, width), jnp.float32),
            rows(3, tok_rows, width),
            pltpu.VMEM((3, 8, tok_rows), jnp.float32),
            rows(3, half * capacity, tok_rows),
            rows(4, 2, tok_rows, half * capacity),
            rows(3, half, capacity, width),
            rows(3, half, capacity, width),
            rows(2, tok_rows, width),
            rows(tok_rows, width),
            rows(tok_rows, width),
            rows(3, quarter, capacity, width),
        ]
        + [dma((bands,))]
        + [dma((len(weights),))] * 3
        + [dma((2,)), dma((2,)), dma((1,)), dma((2,))]
        + [dma((2,)), dma((3, pieces)), dma((2,)), dma((3,))]
        + [dma((3,)), dma((3,)), dma((2,)), dma((2, cuts))]
        + [dma((2,)), dma((cuts,)), dma((1,)), dma((cuts,)), dma((1,)), dma((1,))]
        + [dma((3,)), dma((3, cuts)), dma((4,)), dma((1,))]
        + [pltpu.SemaphoreType.REGULAR],
        compiler_params=pltpu.CompilerParams(
            collective_id=0, has_side_effects=True, vmem_limit_bytes=VMEM_MIB * 1024 * 1024
        ),
        name="layer",
    )(tokens, norm_gain.reshape(1, width), expert_ids.T, route_weights.T, *weights)
    return (held + arrived.astype(jnp.float32)).astype(jnp.bfloat16)


def normalize(tokens, norm_gain):
    values = tokens.astype(jnp.float32)
    factor = lax.rsqrt(jnp.mean(values * values, axis=1, keepdims=True) + epsilon)
    return (values * factor * norm_gain[None, :]).astype(jnp.bfloat16)


def round_term(partial_value):
    return lax.optimization_barrier(partial_value.astype(jnp.bfloat16)).astype(jnp.float32)


def gated_rows(row_block, gate_w, up_w):
    gate_value = jnp.dot(row_block, gate_w, preferred_element_type=jnp.float32)
    up_value = jnp.dot(row_block, up_w, preferred_element_type=jnp.float32)
    return (jax.nn.silu(gate_value) * up_value).astype(jnp.bfloat16)


def sliced_term(hidden, down_w):
    return round_term(jnp.dot(hidden, down_w, preferred_element_type=jnp.float32))


def shared_branch(normed, shared_gate, shared_up, shared_down):
    hidden = gated_rows(lax.all_gather(normed, "tp", axis=0, tiled=True), shared_gate, shared_up)
    return lax.psum_scatter(
        sliced_term(hidden, shared_down).astype(jnp.bfloat16), "tp", scatter_dimension=0, tiled=True
    ).astype(jnp.float32)


def body(
    tokens,
    norm_gain,
    expert_ids,
    route_weights,
    expert_gate,
    expert_up,
    expert_down,
    shared_gate,
    shared_up,
    shared_down,
):
    normed = normalize(tokens, norm_gain)
    tok_rows = tokens.shape[0]
    model_width = tokens.shape[1]
    top_count = expert_ids.shape[1]
    ep_size = lax.axis_size("ep")
    experts = expert_gate.shape[0] * ep_size
    capacity = 3 * tok_rows * top_count // (2 * experts)
    assigned = tok_rows * top_count
    gate_one = expert_gate[0]
    up_one = expert_up[0]
    down_one = expert_down[0]
    flat_ids = expert_ids.reshape(-1)
    onehot = (flat_ids[:, None] == jnp.arange(experts, dtype=jnp.int32)[None, :]).astype(
        jnp.bfloat16
    )
    earlier = (jnp.arange(assigned)[:, None] > jnp.arange(assigned)[None, :]).astype(jnp.bfloat16)
    before_count = jnp.dot(earlier, onehot, preferred_element_type=jnp.float32)
    slot_index = jnp.sum(before_count * onehot.astype(jnp.float32), axis=1).astype(jnp.int32)
    position = flat_ids * capacity + slot_index
    owners = (
        jnp.full((experts * capacity,), tok_rows, jnp.int32)
        .at[position]
        .set(jnp.arange(assigned, dtype=jnp.int32) // top_count)
    )
    padded = jnp.concatenate([normed, jnp.zeros((1, model_width), jnp.bfloat16)], axis=0)
    outgoing = padded[owners].reshape(ep_size, capacity, model_width)
    half_slots = capacity // 2
    split_rows = outgoing.reshape(ep_size, 2, half_slots, model_width)
    results = []
    for portion in range(2):
        received = lax.all_to_all(
            split_rows[:, portion], "ep", split_axis=0, concat_axis=0, tiled=True
        )
        hidden = gated_rows(
            lax.all_gather(
                received.reshape(ep_size * half_slots, model_width), "tp", axis=0, tiled=True
            ),
            gate_one,
            up_one,
        )
        summed = lax.psum_scatter(
            sliced_term(hidden, down_one).astype(jnp.bfloat16),
            "tp",
            scatter_dimension=0,
            tiled=True,
        )
        results.append(
            lax.all_to_all(
                summed.reshape(ep_size, half_slots, model_width),
                "ep",
                split_axis=0,
                concat_axis=0,
                tiled=True,
            )
        )
    returned = jnp.stack(results, axis=1)
    gathered = returned.reshape(experts * capacity, model_width)[position]
    routed = jnp.sum(
        gathered.reshape(tok_rows, top_count, model_width).astype(jnp.float32)
        * route_weights[:, :, None],
        axis=1,
    )
    shared_out = shared_branch(normed, shared_gate, shared_up, shared_down)
    return (routed + shared_out).astype(jnp.bfloat16)


def plan_of(*args):
    peers = lax.axis_size("ep")
    capacity = 3 * args[0].shape[0] * args[2].shape[1] // (2 * peers)
    whole_tiles = capacity % 16 == 0 and peers % 4 == 0 and peers & (peers - 1) == 0
    fits = whole_tiles and lax.axis_size("tp") == 2 and args[4].shape[0] == 1
    return (kernel_body if fits else body)(*args)


def solution(mesh):
    placed = (
        P(("ep", "tp"), None),
        P(),
        P(("ep", "tp"), None),
        P(("ep", "tp"), None),
        P("ep", None, "tp"),
        P("ep", None, "tp"),
        P("ep", "tp", None),
        P(None, "tp"),
        P(None, "tp"),
        P("tp", None),
    )
    return jax.shard_map(
        plan_of, mesh=mesh, in_specs=placed, out_specs=P(("ep", "tp"), None), check_vma=False
    )
```

```python
import functools

import jax
import jax.numpy as jnp
from jax import lax
from jax.experimental import pallas as pl
from jax.experimental.pallas import tpu as pltpu
from jax.sharding import PartitionSpec as P

epsilon = 1e-06
MESH = pl.DeviceIdType.MESH


def toggled(index, step, size):
    total, bit = 0, 1
    while bit < size:
        total = total + bit * ((index // bit + step // bit) % 2)
        bit *= 2
    return total


def gated_sum(rows, gate_w, up_w, down_w):
    total = None
    for half in range(gate_w.shape[0]):
        gate_value = jnp.dot(rows, gate_w[half], preferred_element_type=jnp.float32)
        up_value = jnp.dot(rows, up_w[half], preferred_element_type=jnp.float32)
        hidden = (gate_value / (1.0 + jnp.exp(-gate_value)) * up_value).astype(jnp.bfloat16)
        term = jnp.dot(hidden, down_w[half], preferred_element_type=jnp.float32)
        total = term if total is None else total + term
    return total


def slot_rows(meta, me, steps):
    count = meta.shape[1]
    relative = meta[0:2, :].astype(jnp.int32) ^ me
    step_of = lax.broadcasted_iota(jnp.int32, (steps, count), 0)
    named = (step_of == relative[0:1, :]) | (step_of == relative[1:2, :])
    row_at = lax.broadcasted_iota(jnp.int32, (count, count), 0)
    col_at = lax.broadcasted_iota(jnp.int32, (count, count), 1)
    before = jnp.where(row_at < col_at, 1.0, 0.0).astype(jnp.bfloat16)
    slots = jnp.dot(
        jnp.where(named, 1.0, 0.0).astype(jnp.bfloat16), before, preferred_element_type=jnp.float32
    ).astype(jnp.int32)
    return jnp.where(named, slots, -1)


def picks(slots, steps, capacity):
    slot_at = lax.broadcasted_iota(jnp.int32, (capacity, slots.shape[1]), 0)
    return jnp.concatenate(
        [
            jnp.where(slot_at == slots[step : step + 1, :], 1.0, 0.0).astype(jnp.bfloat16)
            for step in steps
        ],
        axis=0,
    )


def slot_places(meta, me, capacity):
    count = meta.shape[1]
    turned = jnp.transpose(meta)
    relative = turned[:, 0:2].astype(jnp.int32) ^ me
    expert_at = lax.broadcasted_iota(jnp.int32, (count, 128), 1)
    row_at = lax.broadcasted_iota(jnp.int32, (count, count), 0)
    col_at = lax.broadcasted_iota(jnp.int32, (count, count), 1)
    chosen = [expert_at == relative[:, j : j + 1] for j in range(2)]
    after = jnp.where(row_at > col_at, 1.0, 0.0).astype(jnp.bfloat16)
    counted = jnp.dot(
        after,
        jnp.where(chosen[0] | chosen[1], 1.0, 0.0).astype(jnp.bfloat16),
        preferred_element_type=jnp.float32,
    )
    places = [
        relative[:, j : j + 1] * capacity
        + jnp.sum(jnp.where(chosen[j], counted, 0.0), axis=1, keepdims=True).astype(jnp.int32)
        for j in range(2)
    ]
    return places, [turned[:, 2 + j : 3 + j] for j in range(2)]


def weight_matrix(places, weights, first, amount):
    at = lax.broadcasted_iota(jnp.int32, (places[0].shape[0], amount), 1) + first
    scale = jnp.where(at == places[0], weights[0], 0.0) + jnp.where(
        at == places[1], weights[1], 0.0
    )
    upper = scale.astype(jnp.bfloat16)
    return upper, (scale - upper.astype(jnp.float32)).astype(jnp.bfloat16)


def weighted(pair, block):
    return jnp.dot(pair[0], block, preferred_element_type=jnp.float32) + jnp.dot(
        pair[1], block, preferred_element_type=jnp.float32
    )


PIECES = 8
VMEM_MIB = 60
CUTS = 8
OWN_FIRST = (2, 2)
ORDER = (
    "2.0", "2.1", "2.2", "2.3", "0.0", "0.1", "2.4", "2.5", "0.2", "0.3", "2.6", "2.7", "Q", "O.1",
    "0.4", "0.5", "S", "0.6", "0.7", "3.0", "3.1", "3.2", "3.3", "F.0", "O.0", "3.4", "3.5", "A",
    "B", "W.0", "h", "P.0", "4.0", "4.1", "P.2", "m", "4.2", "4.3", "3.6", "3.7", "4.4", "4.5",
    "Y.0", "Y.1", "4.6", "4.7", "Y.2", "Y.3", "Y.4", "Y.5", "Y.6", "Y.7", "F.1", "W.1", "W.2", "a",
    "P.1", "V.0", "V.1", "V.2", "V.3", "V.4", "V.5", "X.0", "X.1", "X.2", "X.3", "V.6", "V.7",
    "X.4", "X.5", "X.6", "X.7", "N", "M",
)


def layer_kernel(
    peers,
    capacity,
    pieces,
    cuts,
    tokens,
    gain,
    expert_ids,
    route_weights,
    expert_gate,
    expert_up,
    expert_down,
    shared_gate,
    shared_up,
    shared_down,
    held,
    sums_in,
    gate_all,
    up_all,
    down_all,
    s_gate_all,
    s_up_all,
    s_down_all,
    raw,
    normed,
    meta,
    outgoing,
    near_in,
    far_in,
    near_out,
    far_out,
    returned,
    total,
    relay_in,
    meta_in,
    picked,
    scales_of,
    relay_out,
    relay_back,
    sums_out,
    pass_in,
    pass_out,
    around,
    token_sems,
    weight_local,
    weight_send,
    weight_recv,
    out_send,
    out_recv,
    back_send,
    back_recv,
    block_send,
    block_recv,
    meta_send,
    meta_recv,
    relay_send,
    relay_recv,
    home_send,
    home_recv,
    sums_send,
    sums_recv,
    pass_send,
    pass_recv,
    middle_send,
    middle_recv,
    side_send,
    side_recv,
    up_send,
    held_send,
    turn,
):
    me = lax.axis_index("ep")
    core = lax.axis_index("tp")
    sibling = 1 - core
    tok_rows, width = normed.shape
    piece, cut = width // pieces, width // cuts
    half, quarter = peers // 2, peers // 4
    inner = ((me // quarter + 1) // 2) % 2
    far_turn, next_turn = half + quarter, quarter
    turns = (half, half + quarter, quarter)

    def at_step(step):
        return (toggled(me, step, peers), core)

    def columns(c):
        return pl.ds(c * piece, piece)

    def cut_columns(c):
        return pl.ds(c * cut, cut)

    def left(source, sem):
        remote(source, source, sem, sem, at_step(1)).wait_send()

    def landed(target, sem):
        remote(target, target, sem, sem, at_step(1)).wait_recv()

    def on_inner(action):
        pl.when(inner == 1)(action)

    def on_outer(action):
        pl.when(inner == 0)(action)

    def remote(source, target, send, recv, place):
        return pltpu.make_async_remote_copy(
            src_ref=source,
            dst_ref=target,
            send_sem=send,
            recv_sem=recv,
            device_id=place,
            device_id_type=MESH,
        )

    barrier = pltpu.get_barrier_semaphore()
    greeted = [step for step in range(1, half)] + [half, far_turn]
    pl.semaphore_signal(barrier, inc=1, device_id=(me, sibling), device_id_type=MESH)
    for step in greeted:
        pl.semaphore_signal(barrier, inc=1, device_id=at_step(step), device_id_type=MESH)
    bands = token_sems.shape[0]
    band = tok_rows // bands
    fetched = [
        pltpu.make_async_copy(
            tokens.at[pl.ds(i * band, band)], raw.at[pl.ds(i * band, band)], token_sems.at[i]
        )
        for i in range(bands)
    ]
    for copy in fetched:
        copy.start()
    sources = (
        (shared_gate, s_gate_all),
        (shared_up, s_up_all),
        (shared_down, s_down_all),
        (expert_gate, gate_all),
        (expert_up, up_all),
        (expert_down, down_all),
    )
    local = [
        pltpu.make_async_copy(source, target.at[core], weight_local.at[i])
        for i, (source, target) in enumerate(sources)
    ]
    swaps = [
        remote(source, target.at[core], weight_send.at[i], weight_recv.at[i], (me, sibling))
        for i, (source, target) in enumerate(sources)
    ]

    def normalize_rows():
        for i in range(bands):
            fetched[i].wait()
            at = pl.ds(i * band, band)
            values = raw[at].astype(jnp.float32)
            factor = lax.rsqrt(jnp.mean(values * values, axis=1, keepdims=True) + epsilon)
            normed[at] = (values * factor * gain[...]).astype(jnp.bfloat16)

    with jax.named_scope("norm"):
        normalize_rows()
    meta[0:2] = expert_ids[...].astype(jnp.float32)
    meta[2:4] = route_weights[...]
    meta[4:8] = jnp.zeros((4, tok_rows), jnp.float32)

    def meta_copy(side):
        step = {0: half, 1: far_turn, 2: next_turn}[side]
        number = 1 if side == 0 else 0
        return remote(
            meta, meta_in.at[side], meta_send.at[number], meta_recv.at[side], at_step(step)
        )

    def block_copy(side, c):
        return remote(
            normed.at[:, columns(c)],
            relay_in.at[side, :, columns(c)],
            block_send.at[0],
            block_recv.at[side, c],
            at_step(far_turn if side == 1 else next_turn),
        )

    def forward(c):
        return remote(
            relay_in.at[2, :, columns(c)],
            relay_in.at[0, :, columns(c)],
            block_send.at[1],
            block_recv.at[0, c],
            at_step(far_turn),
        )

    def dispatch(step):
        group = step // quarter
        return remote(
            outgoing.at[step],
            near_in.at[step],
            out_send.at[group],
            out_recv.at[group],
            at_step(step),
        )

    def give_back(step):
        return remote(
            near_out.at[step],
            returned.at[step],
            back_send.at[0],
            back_recv.at[0],
            at_step(step),
        )

    def relay(side, k, c):
        target = near_in.at[k + quarter] if side == 2 else far_in.at[side, k % quarter]
        return remote(
            relay_out.at[side, k, :, columns(c)],
            target.at[:, columns(c)],
            relay_send.at[side],
            relay_recv.at[side],
            at_step(k),
        )

    def home(side, j, c):
        k = j + quarter * (1 - inner)
        return remote(
            far_out.at[side, j, :, cut_columns(c)],
            relay_back.at[side, k, :, cut_columns(c)],
            home_send.at[side],
            home_recv.at[side, c],
            at_step(k),
        )

    def sideways(side, j, c):
        source = near_out.at[quarter + j] if side == 2 else far_out.at[side, j]
        return remote(
            source.at[:, cut_columns(c)],
            around.at[side, j, :, cut_columns(c)],
            side_send.at[side],
            side_recv.at[side, c],
            at_step(j),
        )

    def upward(side, j, c):
        if side == 2:
            target, recv = returned.at[quarter + j], back_recv.at[1]
        else:
            target, recv = relay_back.at[side, quarter + j], home_recv.at[side, c]
        return remote(
            around.at[side, j, :, cut_columns(c)],
            target.at[:, cut_columns(c)],
            up_send.at[side],
            recv,
            at_step(next_turn),
        )

    def straight(c):
        return remote(
            near_out.at[quarter, :, cut_columns(c)],
            returned.at[quarter, :, cut_columns(c)],
            up_send.at[3],
            back_recv.at[1],
            at_step(next_turn),
        )

    def middle(j):
        return remote(
            near_out.at[quarter + j],
            relay_back.at[2, j],
            middle_send.at[0],
            middle_recv.at[0],
            at_step(j),
        )

    def sums(side, c):
        target = pass_in if side == 0 else sums_in
        return remote(
            sums_out.at[side, :, cut_columns(c)],
            target.at[:, cut_columns(c)],
            sums_send.at[side],
            pass_recv.at[c] if side == 0 else sums_recv.at[c],
            at_step(far_turn),
        )

    def sums_on(c):
        return remote(
            pass_out.at[:, cut_columns(c)],
            sums_in.at[:, cut_columns(c)],
            pass_send.at[0],
            sums_recv.at[c],
            at_step(next_turn),
        )

    def start_own(which, first, last):
        if last > first:

            @pl.when(core == which)
            def _():
                for c in range(first, last):
                    block_copy(1, c).start()

    def start_block():
        for c in range(pieces):
            block_copy(2, c).start()

    with jax.named_scope("meet"):
        pl.semaphore_wait(barrier, len(greeted) + 1)

    @pl.when(inner == 1)
    def _():
        meta_copy(1).start()
        start_own(1, 0, OWN_FIRST[1])

    @pl.when(inner == 0)
    def _():
        meta_copy(2).start()
        meta_copy(0).start()
        pl.when(core == 0)(start_block)

    for copy in local:
        copy.start()
    slots = slot_rows(meta[...], me, half)

    def send_slots(first):
        rows = jnp.dot(
            picks(slots, range(first, first + quarter), capacity),
            normed[...],
            preferred_element_type=jnp.float32,
        ).astype(jnp.bfloat16)
        for i in range(quarter):
            block = rows[i * capacity : (i + 1) * capacity]
            if first + i == 0:
                near_in[0] = block
            else:
                outgoing[first + i] = block
                dispatch(first + i).start()

    on_inner(lambda: send_slots(quarter))
    send_slots(0)
    for copy in swaps:
        copy.start()

    @pl.when((inner == 0) & (core == 0))
    def _():
        left(normed, block_send.at[0])
        pl.semaphore_signal(turn, inc=1, device_id=(me, sibling), device_id_type=MESH)

    @pl.when((inner == 0) & (core == 1))
    def _():
        pl.semaphore_wait(turn, 1)
        start_block()

    def open_side(side):
        landed(meta_in.at[side], meta_recv.at[side])
        reach = quarter if side == 2 else half
        picked[side, : reach * capacity] = picks(
            slot_rows(meta_in[side], me, half), range(reach), capacity
        )

    def pass_on(side, c):
        if c == 0:
            open_side(side)
        reach = quarter if side == 2 else half
        landed(relay_in.at[side, :, columns(c)], block_recv.at[side, c])
        if side == 2:
            forward(c).start()
        rows = jnp.dot(
            picked[side, : reach * capacity],
            relay_in[side, :, columns(c)],
            preferred_element_type=jnp.float32,
        ).astype(jnp.bfloat16)
        if side == 2:
            near_in[quarter, :, columns(c)] = rows[:capacity]
        else:
            far_in[side, 0, :, columns(c)] = rows[:capacity]
        for k in range(reach - 1, 0, -1):
            relay_out[side, k, :, columns(c)] = rows[k * capacity : (k + 1) * capacity]
            relay(side, k, c).start()

    def near(group):
        steps = range(group * quarter, (group + 1) * quarter)
        if group == 0:
            landed(near_in.at[pl.ds(1, quarter - 1)], out_recv.at[0])
        else:
            on_outer(lambda: landed(near_in.at[pl.ds(quarter, quarter)], out_recv.at[1]))
            on_inner(
                lambda: landed(near_in.at[pl.ds(quarter + 1, quarter - 1)], relay_recv.at[2])
            )

        block = near_in[group * quarter : (group + 1) * quarter].reshape(quarter * capacity, width)
        out = gated_sum(block, gate_all, up_all, down_all).astype(jnp.bfloat16)
        for i, step in enumerate(steps):
            part = out[i * capacity : (i + 1) * capacity]
            if step == 0:
                returned[0] = part
            else:
                near_out[step] = part

    def near_send():
        for step in range(1, quarter):
            give_back(step).start()

    def middle_send_all():
        relay_back[2, 0] = near_out[quarter]
        for j in range(1, quarter):
            middle(j).start()

    def near_sideways():
        for c in range(cuts):
            straight(c).start()
            for j in range(1, quarter):
                sideways(2, j, c).start()

    def pass_up(side):
        for c in range(cuts):
            with jax.named_scope("up_" + str(c)):
                gathered = around.at[side, pl.ds(1, quarter - 1), :, cut_columns(c)]
                landed(gathered, side_recv.at[side, c])
                for j in range(1, quarter):
                    upward(side, j, c).start()

    def far(side):
        on_outer(lambda: landed(far_in.at[side], relay_recv.at[side]))
        on_inner(lambda: landed(far_in.at[side, pl.ds(1, quarter - 1)], relay_recv.at[side]))
        block = far_in[side].reshape(quarter * capacity, width)
        out = gated_sum(block, gate_all, up_all, down_all).astype(jnp.bfloat16)
        far_out[side] = out.reshape(quarter, capacity, width)

        @pl.when(inner == 1)
        def _():
            relay_back[side, 0] = far_out[side, 0]
            for c in range(cuts):
                for j in range(quarter - 1, 0, -1):
                    home(side, j, c).start()

        @pl.when(inner == 0)
        def _():
            for c in range(cuts):
                for j in range(1, quarter):
                    sideways(side, j, c).start()
                home(side, 0, c).start()

    def prepare(side, source, reach):
        places, scales = slot_places(source[...], me, capacity)
        upper, lower = weight_matrix(places, scales, 0, reach * capacity)
        scales_of[side, 0, :, : reach * capacity] = upper
        scales_of[side, 1, :, : reach * capacity] = lower

    def weighted_by(side, reach, block):
        span = reach * capacity
        pair = (scales_of[side, 0, :, :span], scales_of[side, 1, :, :span])
        return weighted(pair, block.reshape(span, block.shape[-1]))

    def send_sums(side, c):
        landed(relay_back.at[side, pl.ds(1, half - 1), :, cut_columns(c)], home_recv.at[side, c])
        block = relay_back[side, :, :, cut_columns(c)]
        sums_out[side, :, cut_columns(c)] = weighted_by(side, half, block).astype(jnp.bfloat16)
        sums(side, c).start()

    def send_on(c):
        if c == 0:
            landed(relay_back.at[2, pl.ds(1, quarter - 1)], middle_recv.at[0])
        block = relay_back[2, :quarter, :, cut_columns(c)]
        own = weighted_by(2, quarter, block)
        at = cut_columns(c)
        landed(pass_in.at[:, at], pass_recv.at[c])
        pass_out[:, at] = (own + pass_in[:, at].astype(jnp.float32)).astype(jnp.bfloat16)
        sums_on(c).start()

    def shared():
        for i in range(len(sources)):
            local[i].wait()
            swaps[i].wait()
        total[...] = gated_sum(normed[...], s_gate_all, s_up_all, s_down_all)

    def near_total():
        prepare(3, meta, half)
        landed(returned.at[pl.ds(1, quarter - 1)], back_recv.at[0])
        total[...] += weighted_by(3, quarter, returned[:quarter])

    def outer_total():
        span = quarter * capacity
        landed(returned.at[pl.ds(quarter, quarter)], back_recv.at[1])
        pair = (scales_of[3, 0, :, span:], scales_of[3, 1, :, span:])
        total[...] += weighted(pair, returned[quarter:].reshape(span, width))

    actions = {
        "S": shared,
        "A": lambda: near(0),
        "B": lambda: near(1),
        "a": near_send,
        "m": lambda: on_inner(middle_send_all),
        "h": lambda: on_outer(near_sideways),
        "N": near_total,
        "Q": lambda: on_inner(lambda: start_own(0, 0, OWN_FIRST[0])),
        "M": lambda: on_inner(outer_total),
    }
    numbered = {
        "0": lambda c: on_inner(lambda: pass_on(0, c)),
        "1": lambda c: on_inner(lambda: pass_on(1, c)),
        "2": lambda c: on_inner(lambda: pass_on(2, c)),
        "3": lambda c: pl.when((inner == 1) & (core == 1))(lambda: pass_on(1, c)),
        "4": lambda c: pl.when((inner == 1) & (core == 0))(lambda: pass_on(1, c)),
        "O": lambda which: on_inner(lambda: start_own(which, OWN_FIRST[which], pieces)),
        "F": far,
        "W": lambda side: on_outer(lambda: pass_up(side)),
        "P": lambda side: on_inner(
            lambda: prepare(side, meta_in.at[side], quarter if side == 2 else half)
        ),
        "V": lambda c: on_inner(lambda: send_on(c)),
        "X": lambda c: on_inner(lambda: send_sums(1, c)),
        "Y": lambda c: on_inner(lambda: send_sums(0, c)),
    }
    for name in ORDER:
        with jax.named_scope("do_" + name):
            if name in actions:
                actions[name]()
            else:
                numbered[name[0]](int(name[2:]))

    keep = pltpu.make_async_copy(total, held, held_send.at[0])
    keep.start()
    with jax.named_scope("settle"):
        left(outgoing.at[pl.ds(1, quarter - 1)], out_send.at[0])
        left(near_out.at[pl.ds(1, quarter - 1)], back_send.at[0])

        @pl.when((inner == 1) | (core == 1))
        def _():
            left(normed, block_send.at[0])

        @pl.when(inner == 0)
        def _():
            left(meta, meta_send.at[0])
            left(meta, meta_send.at[1])
            left(near_out.at[quarter], up_send.at[3])
            for side in range(2):
                left(far_out.at[side, 0], home_send.at[side])
            for side in range(3):
                left(around.at[side, pl.ds(1, quarter - 1)], side_send.at[side])
                left(around.at[side, pl.ds(1, quarter - 1)], up_send.at[side])

        @pl.when(inner == 1)
        def _():
            left(meta, meta_send.at[0])
            left(outgoing.at[pl.ds(quarter, quarter)], out_send.at[1])
            left(near_out.at[pl.ds(1, quarter - 1)], middle_send.at[0])
            left(normed, block_send.at[1])
            for side in range(2):
                left(far_out.at[side, pl.ds(1, quarter - 1)], home_send.at[side])
                left(relay_out.at[side, pl.ds(1, half - 1)], relay_send.at[side])
                left(normed, sums_send.at[side])
            left(relay_out.at[2, pl.ds(1, quarter - 1)], relay_send.at[2])
            left(normed, pass_send.at[0])

        keep.wait()
        for c in range(cuts):
            landed(sums_in.at[:, cut_columns(c)], sums_recv.at[c])


def kernel_body(
    tokens,
    norm_gain,
    expert_ids,
    route_weights,
    expert_gate,
    expert_up,
    expert_down,
    shared_gate,
    shared_up,
    shared_down,
):
    peers = lax.axis_size("ep")
    halves = lax.axis_size("tp")
    tok_rows, width = tokens.shape
    capacity = 3 * tok_rows * expert_ids.shape[1] // (2 * peers)
    half, quarter, pieces, cuts, bands = peers // 2, peers // 4, PIECES, CUTS, 4
    vmem = pl.BlockSpec(memory_space=pltpu.VMEM)
    anywhere = pl.BlockSpec(memory_space=pl.ANY)
    weights = (
        expert_gate[0],
        expert_up[0],
        expert_down[0],
        shared_gate,
        shared_up,
        shared_down,
    )

    def rows(*shape):
        return pltpu.VMEM(shape, jnp.bfloat16)

    dma = pltpu.SemaphoreType.DMA
    held, arrived = pl.pallas_call(
        functools.partial(layer_kernel, peers, capacity, pieces, cuts),
        out_shape=[
            jax.ShapeDtypeStruct((tok_rows, width), jnp.float32),
            jax.ShapeDtypeStruct((tok_rows, width), jnp.bfloat16),
        ],
        in_specs=[anywhere] + [vmem] * 3 + [anywhere] * 6,
        out_specs=[anywhere] * 2,
        scratch_shapes=[pltpu.VMEM((halves,) + w.shape, w.dtype) for w in weights]
        + [
            rows(tok_rows, width),
            rows(tok_rows, width),
            pltpu.VMEM((8, tok_rows), jnp.float32),
            rows(half, capacity, width),
            rows(half, capacity, width),
            rows(2, quarter, capacity, width),
            rows(half, capacity, width),
            rows(2, quarter, capacity, width),
            rows(half, capacity, width),
            pltpu.VMEM((tok_rows, width), jnp.float32),
            rows(3, tok_rows, width),
            pltpu.VMEM((3, 8, tok_rows), jnp.float32),
            rows(3, half * capacity, tok_rows),
            rows(4, 2, tok_rows, half * capacity),
            rows(3, half, capacity, width),
            rows(3, half, capacity, width),
            rows(2, tok_rows, width),
            rows(tok_rows, width),
            rows(tok_rows, width),
            rows(3, quarter, capacity, width),
        ]
        + [dma((bands,))]
        + [dma((len(weights),))] * 3
        + [dma((2,)), dma((2,)), dma((1,)), dma((2,))]
        + [dma((2,)), dma((3, pieces)), dma((2,)), dma((3,))]
        + [dma((3,)), dma((3,)), dma((2,)), dma((2, cuts))]
        + [dma((2,)), dma((cuts,)), dma((1,)), dma((cuts,)), dma((1,)), dma((1,))]
        + [dma((3,)), dma((3, cuts)), dma((4,)), dma((1,))]
        + [pltpu.SemaphoreType.REGULAR],
        compiler_params=pltpu.CompilerParams(
            collective_id=0, has_side_effects=True, vmem_limit_bytes=VMEM_MIB * 1024 * 1024
        ),
        name="layer",
    )(tokens, norm_gain.reshape(1, width), expert_ids.T, route_weights.T, *weights)
    return (held + arrived.astype(jnp.float32)).astype(jnp.bfloat16)


def normalize(tokens, norm_gain):
    values = tokens.astype(jnp.float32)
    factor = lax.rsqrt(jnp.mean(values * values, axis=1, keepdims=True) + epsilon)
    return (values * factor * norm_gain[None, :]).astype(jnp.bfloat16)


def round_term(partial_value):
    return lax.optimization_barrier(partial_value.astype(jnp.bfloat16)).astype(jnp.float32)


def gated_rows(row_block, gate_w, up_w):
    gate_value = jnp.dot(row_block, gate_w, preferred_element_type=jnp.float32)
    up_value = jnp.dot(row_block, up_w, preferred_element_type=jnp.float32)
    return (jax.nn.silu(gate_value) * up_value).astype(jnp.bfloat16)


def sliced_term(hidden, down_w):
    return round_term(jnp.dot(hidden, down_w, preferred_element_type=jnp.float32))


def shared_branch(normed, shared_gate, shared_up, shared_down):
    hidden = gated_rows(lax.all_gather(normed, "tp", axis=0, tiled=True), shared_gate, shared_up)
    return lax.psum_scatter(
        sliced_term(hidden, shared_down).astype(jnp.bfloat16), "tp", scatter_dimension=0, tiled=True
    ).astype(jnp.float32)


def body(
    tokens,
    norm_gain,
    expert_ids,
    route_weights,
    expert_gate,
    expert_up,
    expert_down,
    shared_gate,
    shared_up,
    shared_down,
):
    normed = normalize(tokens, norm_gain)
    tok_rows = tokens.shape[0]
    model_width = tokens.shape[1]
    top_count = expert_ids.shape[1]
    ep_size = lax.axis_size("ep")
    experts = expert_gate.shape[0] * ep_size
    capacity = 3 * tok_rows * top_count // (2 * experts)
    assigned = tok_rows * top_count
    gate_one = expert_gate[0]
    up_one = expert_up[0]
    down_one = expert_down[0]
    flat_ids = expert_ids.reshape(-1)
    onehot = (flat_ids[:, None] == jnp.arange(experts, dtype=jnp.int32)[None, :]).astype(
        jnp.bfloat16
    )
    earlier = (jnp.arange(assigned)[:, None] > jnp.arange(assigned)[None, :]).astype(jnp.bfloat16)
    before_count = jnp.dot(earlier, onehot, preferred_element_type=jnp.float32)
    slot_index = jnp.sum(before_count * onehot.astype(jnp.float32), axis=1).astype(jnp.int32)
    position = flat_ids * capacity + slot_index
    owners = (
        jnp.full((experts * capacity,), tok_rows, jnp.int32)
        .at[position]
        .set(jnp.arange(assigned, dtype=jnp.int32) // top_count)
    )
    padded = jnp.concatenate([normed, jnp.zeros((1, model_width), jnp.bfloat16)], axis=0)
    outgoing = padded[owners].reshape(ep_size, capacity, model_width)
    half_slots = capacity // 2
    split_rows = outgoing.reshape(ep_size, 2, half_slots, model_width)
    results = []
    for portion in range(2):
        received = lax.all_to_all(
            split_rows[:, portion], "ep", split_axis=0, concat_axis=0, tiled=True
        )
        hidden = gated_rows(
            lax.all_gather(
                received.reshape(ep_size * half_slots, model_width), "tp", axis=0, tiled=True
            ),
            gate_one,
            up_one,
        )
        summed = lax.psum_scatter(
            sliced_term(hidden, down_one).astype(jnp.bfloat16),
            "tp",
            scatter_dimension=0,
            tiled=True,
        )
        results.append(
            lax.all_to_all(
                summed.reshape(ep_size, half_slots, model_width),
                "ep",
                split_axis=0,
                concat_axis=0,
                tiled=True,
            )
        )
    returned = jnp.stack(results, axis=1)
    gathered = returned.reshape(experts * capacity, model_width)[position]
    routed = jnp.sum(
        gathered.reshape(tok_rows, top_count, model_width).astype(jnp.float32)
        * route_weights[:, :, None],
        axis=1,
    )
    shared_out = shared_branch(normed, shared_gate, shared_up, shared_down)
    return (routed + shared_out).astype(jnp.bfloat16)


def plan_of(*args):
    peers = lax.axis_size("ep")
    capacity = 3 * args[0].shape[0] * args[2].shape[1] // (2 * peers)
    whole_tiles = capacity % 16 == 0 and peers % 4 == 0 and peers & (peers - 1) == 0
    fits = whole_tiles and lax.axis_size("tp") == 2 and args[4].shape[0] == 1
    return (kernel_body if fits else body)(*args)


def solution(mesh):
    placed = (
        P(("ep", "tp"), None),
        P(),
        P(("ep", "tp"), None),
        P(("ep", "tp"), None),
        P("ep", None, "tp"),
        P("ep", None, "tp"),
        P("ep", "tp", None),
        P(None, "tp"),
        P(None, "tp"),
        P("tp", None),
    )
    return jax.shard_map(
        plan_of, mesh=mesh, in_specs=placed, out_specs=P(("ep", "tp"), None), check_vma=False
    )
```
